128 devices in a mesh: fs: 16 (over z, x), tp: 8 (over y, core).
Axes of the slice: x: 4, y: 4, z: 4, core: 2. Of those that a mesh axis runs over, the one named last changes fastest.
Arguments:
- saved_input: bfloat16 [49152, 2048], P('fs'), may hold values from -6 to 6
- proj_cot: bfloat16 [3, 49152, 2048], P(None, 'fs', 'tp'), may hold values from -0.02734375 to 0.02734375
- log_cache: float32 [16, 49152], P(None, 'fs'), as said below
- cache_cot: float32 [16, 49152], P(None, 'fs'), may hold values from -0.02734375 to 0.02734375
- proj_master: float32 [3, 2048, 2048], P(None, 'fs', 'tp'), may hold values from -0.125 to 0.125
- factors: bfloat16 [3, 2048, 256], P(None, 'fs'), may hold values from -0.125 to 0.125
- first_moment: float32 [3, 256, 2048], P(None, None, 'tp'), may hold values from -6 to 6
- second_moment: float32 [3, 256, 2048], P(None, None, 'tp'), may hold values from 0.01 to 10
- gate_master: float32 [16, 2048], replicated, may hold values from -0.125 to 0.125
- gate_first: float32 [16, 2048], replicated, may hold values from -6 to 6
- gate_second: float32 [16, 2048], replicated, may hold values from 0.1 to 3
Outputs:
- proj_step: float32 [3, 2048, 2048], P(None, 'fs', 'tp')
- proj_new: float32 [3, 2048, 2048], P(None, 'fs', 'tp')
- proj_copy: bfloat16 [3, 2048, 2048], P(None, None, 'tp')
- first_new: float32 [3, 256, 2048], P(None, None, 'tp')
- second_new: float32 [3, 256, 2048], P(None, None, 'tp')
- gate_new: float32 [16, 2048], replicated
- gate_copy: bfloat16 [16, 2048], replicated
- gate_first_new: float32 [16, 2048], replicated
- gate_second_new: float32 [16, 2048], replicated
The draws below stay inside these ranges and needn't reach their ends.
Inputs may be any that keep to these rules, and one draw needn't show every extreme that they name: `log_cache`: each head's values never rise along positions.
All inputs are finite; a program needn't handle non-finite values.
Results may differ from the reference program's by a relative error of at most 0.0004.
Values may be sent and summed in bfloat16 or wider, within the bound.
No kernel may reach another device: no remote copies, remote signals or barrier semaphores. Data moves between devices by JAX's collectives and lax.ppermute only.
A program may use at most 128 MiB of HBM per device.

```python
import math
import jax
import jax.numpy as jnp
from jax import lax

D = 2048
ATTENTION_HEADS = 16
RANK = 256
ROLES = 3
TOK_DEV = 3072
W = 2048
SEQUENCE_TOKENS = 49152


def draw_log_cache(key, part):
    keys = jax.random.split(key, 7)
    order = jax.random.permutation(keys[0], ATTENTION_HEADS)
    slow_decay = order < ATTENTION_HEADS // 2
    total = jnp.exp(jax.random.uniform(keys[1], (ATTENTION_HEADS, 1), jnp.float32, math.log(0.3), math.log(1.0)))
    fast_rate = jnp.exp(jax.random.uniform(keys[2], (ATTENTION_HEADS, 1), jnp.float32, math.log(0.01), math.log(1.0 / 30.0)))
    learning_rate = jnp.where(slow_decay[:, None], total / SEQUENCE_TOKENS, fast_rate)
    blocks = SEQUENCE_TOKENS // TOK_DEV
    block_multiplier = jnp.exp(jax.random.uniform(keys[3], (ATTENTION_HEADS, blocks), jnp.float32, math.log(0.5), math.log(2.0)))
    block_multiplier = jnp.repeat(block_multiplier, TOK_DEV, axis=1)
    coarse_estimate = jnp.exp(jax.random.uniform(keys[4], (ATTENTION_HEADS, SEQUENCE_TOKENS), jnp.float32, -0.7, 0.7))
    chosen_locations = jax.random.randint(keys[5], (ATTENTION_HEADS, 3), 0, SEQUENCE_TOKENS)
    layer_depth = jax.random.uniform(keys[6], (ATTENTION_HEADS, 3), jnp.float32, 0.22, 0.5)
    target_positions = jnp.arange(SEQUENCE_TOKENS)
    sudden_spike = jnp.zeros((ATTENTION_HEADS, SEQUENCE_TOKENS), jnp.float32)
    for position_index in range(3):
        sudden_spike = sudden_spike + jnp.where(target_positions[None, :] == chosen_locations[:, position_index:position_index + 1], layer_depth[:, position_index:position_index + 1], 0.0)
    gate_logarithm = -(learning_rate * block_multiplier * coarse_estimate) - sudden_spike * slow_decay[:, None].astype(jnp.float32)
    return jnp.cumsum(gate_logarithm, axis=1)


def draw_second_moment(key, part):
    lower, upper, fall = (1.0, 10.0, 10.0)
    base = jnp.exp(jax.random.uniform(key, (ROLES, RANK, W), jnp.float32, math.log(lower), math.log(upper)))
    column = jnp.arange(W, dtype=jnp.float32) / W
    return base * jnp.power(fall, -column)[None, None, :]


def block_levels(rng, dims, shards, smallest, largest):
    level, own = 1.0, jax.random.fold_in(rng, 6)
    for position, parts in shards:
        draws = jnp.exp(jax.random.uniform(jax.random.fold_in(own, position), (parts,), jnp.float32, smallest / len(shards), largest / len(shards)))
        level = level * jnp.repeat(draws, dims[position] // parts).reshape([-1 if axis == position else 1 for axis in range(len(dims))])
    return level


def scatter_about(stream_key, extent, spread, reach, cuts=(), held_as=jnp.bfloat16):
    factor_of = block_levels(stream_key, extent, cuts, -0.22, 0.18) if cuts else 1.0
    drawn = jax.random.normal(stream_key, extent, jnp.float32) * spread * factor_of
    return jnp.minimum(jnp.maximum(drawn, -reach), reach).astype(held_as)


def setup_inputs(seed: int = 0) -> dict:
    splits = jax.random.split(jax.random.key(seed), 12)
    saved_input = scatter_about(splits[0], (SEQUENCE_TOKENS, D), 1.0, 6.0, ((0, 16),))
    proj_cot = scatter_about(splits[1], (ROLES, SEQUENCE_TOKENS, W), SEQUENCE_TOKENS ** -0.5, 0.02734375, ((1, 16), (2, 8)))
    log_cache = draw_log_cache(jax.random.fold_in(splits[11], 71), 0)
    cache_cot = scatter_about(splits[3], (ATTENTION_HEADS, SEQUENCE_TOKENS), SEQUENCE_TOKENS ** -0.5, 0.02734375, ((1, 16),), jnp.float32)
    proj_master = scatter_about(splits[4], (ROLES, D, W), D ** -0.5, 0.125, ((1, 16), (2, 8)), jnp.float32)
    factors = scatter_about(splits[5], (ROLES, D, RANK), D ** -0.5, 0.125, ((1, 16),))
    first_moment = scatter_about(splits[6], (ROLES, RANK, W), 1.0, 6.0, ((2, 8),), jnp.float32)
    second_moment = draw_second_moment(jax.random.fold_in(splits[11], 71), 0)
    gate_master = scatter_about(splits[8], (ATTENTION_HEADS, D), D ** -0.5, 0.125, (), jnp.float32)
    gate_first = scatter_about(splits[9], (ATTENTION_HEADS, D), 1.0, 6.0, (), jnp.float32)
    gate_second = jnp.clip(jnp.exp(jax.random.uniform(splits[10], (ATTENTION_HEADS, D), jnp.float32, math.log(0.1), math.log(3.0))), 0.1, 3.0)
    return {"saved_input": saved_input, "proj_cot": proj_cot, "log_cache": log_cache, "cache_cot": cache_cot, "proj_master": proj_master, "factors": factors, "first_moment": first_moment, "second_moment": second_moment, "gate_master": gate_master, "gate_first": gate_first, "gate_second": gate_second}


BETA_ONE = 0.8
BETA_TWO = 0.9
LEARN = 0.001

def reference(saved_input, proj_cot, log_cache, cache_cot, proj_master, factors, first_moment, second_moment, gate_master, gate_first, gate_second):
    lows = []
    for role in range(ROLES):
        grad = jnp.dot(saved_input.T, proj_cot[role], preferred_element_type=jnp.float32)
        lows.append(jnp.dot(factors[role].astype(jnp.float32).T, grad, precision=lax.Precision.HIGHEST))
    low = jnp.stack(lows)
    first_new = BETA_ONE * first_moment + (1.0 - BETA_ONE) * low
    second_new = BETA_TWO * second_moment + (1.0 - BETA_TWO) * low * low
    direction = first_new / jnp.sqrt(second_new)
    scale = lax.rsqrt(jnp.mean(direction * direction) + 1e-06)
    product = jnp.einsum('rdk,rkw->rdw', factors.astype(jnp.float32), direction, precision=lax.Precision.HIGHEST)
    proj_step = scale * product
    proj_new = proj_master - LEARN * proj_step
    proj_copy = proj_new.astype(jnp.bfloat16)
    previous = jnp.concatenate([jnp.zeros((ATTENTION_HEADS, 1), jnp.float32), log_cache[:, :-1]], axis=1)
    gate_logarithm = log_cache - previous
    later = jnp.flip(jnp.cumsum(jnp.flip(cache_cot, 1), axis=1), 1)
    gate_cot = (later * -jnp.expm1(gate_logarithm)).astype(jnp.bfloat16)
    gate_grad = jnp.dot(gate_cot, saved_input, preferred_element_type=jnp.float32)
    gate_first_new = BETA_ONE * gate_first + (1.0 - BETA_ONE) * gate_grad
    gate_second_new = BETA_TWO * gate_second + (1.0 - BETA_TWO) * gate_grad * gate_grad
    gate_new = gate_master - LEARN * gate_first_new / jnp.sqrt(gate_second_new)
    gate_copy = gate_new.astype(jnp.bfloat16)
    return (proj_step, proj_new, proj_copy, first_new, second_new, gate_new, gate_copy, gate_first_new, gate_second_new)
```

```python
import functools

import jax
import jax.numpy as jnp
from jax import lax
from jax.experimental import pallas as pl
from jax.experimental.pallas import tpu as pltpu
from jax.sharding import Mesh
from jax.sharding import PartitionSpec as P

BETA_ONE = 0.8
BETA_TWO = 0.9
LEARN = 0.001
FS = ("z", "x")
TP = ("y", "c")


def from_everyone(x, axis):
    copies = jnp.broadcast_to(x, (lax.axis_size(axis), *x.shape))
    return lax.all_to_all(copies, axis, split_axis=0, concat_axis=0, tiled=True)


def gate_kernel(me_ref, log_ref, cot_ref, ends_ref, out_ref):
    me = me_ref[0]
    heads, length = log_ref.shape
    ends = ends_ref[...]
    source = lax.broadcasted_iota(jnp.int32, ends.shape, 0)
    after = jnp.sum(jnp.where(source > me, ends, 0.0), axis=0, keepdims=True)
    before = jnp.sum(jnp.where(source == me - 1, ends, 0.0), axis=0, keepdims=True)
    lane = lax.broadcasted_iota(jnp.int32, (heads, ends.shape[1]), 1)
    row = lax.broadcasted_iota(jnp.int32, (heads, ends.shape[1]), 0)
    carried = jnp.sum(jnp.where(lane == row, after, 0.0), axis=1, keepdims=True)
    edge = jnp.sum(jnp.where(lane == row + heads, before, 0.0), axis=1, keepdims=True)
    place = lax.broadcasted_iota(jnp.int32, (heads, length), 1)
    total = cot_ref[...]
    step = 1
    while step < length:
        total = total + jnp.where(place < length - step, pltpu.roll(total, length - step, 1), 0.0)
        step *= 2
    log = log_ref[...]
    previous = jnp.where(place == 0, edge, pltpu.roll(log, 1, 1))
    delta = log - previous
    closed = -jnp.tanh(0.5 * delta) * (jnp.exp(delta) + 1.0)
    out_ref[...] = ((total + carried) * closed).astype(out_ref.dtype)


def gate_cotangent(log_cache, cache_cot, ends, me):
    heads, length = log_cache.shape
    vmem = pl.BlockSpec(memory_space=pltpu.VMEM)
    return pl.pallas_call(
        gate_kernel,
        out_shape=jax.ShapeDtypeStruct((heads, length), jnp.bfloat16),
        in_specs=[pl.BlockSpec(memory_space=pltpu.SMEM), vmem, vmem, vmem],
        out_specs=vmem,
        cost_estimate=pl.CostEstimate(
            flops=40 * heads * length, bytes_accessed=10 * heads * length, transcendentals=0
        ),
        name="gate_cotangent",
    )(me.reshape(1).astype(jnp.int32), log_cache, cache_cot, ends)


def local(
    saved_input,
    proj_cot,
    log_cache,
    cache_cot,
    proj_master,
    factors,
    first_moment,
    second_moment,
    gate_master,
    gate_first,
    gate_second,
):
    roles, rows, rank = factors.shape
    heads = log_cache.shape[0]
    width = proj_cot.shape[2]
    peers = lax.axis_size(FS)
    me = lax.axis_index(FS)
    core = lax.axis_index("c")
    cores = lax.axis_size("c")
    half = rank // cores

    ends = jnp.concatenate([jnp.sum(cache_cot, axis=1), log_cache[:, -1]])
    ends = from_everyone(ends.reshape(1, 1, -1), FS).reshape(peers, -1)
    ends = jnp.pad(ends, ((0, 0), (0, 128 - ends.shape[1])))
    own_factors = lax.dynamic_slice_in_dim(factors, core * half, half, axis=2)
    near = from_everyone(own_factors, FS)
    far = lax.ppermute(near, "c", [(0, 1), (1, 0)])

    grad = jnp.einsum("td,rtw->rdw", saved_input, proj_cot, preferred_element_type=jnp.float32)
    upper = lax.optimization_barrier(grad.astype(jnp.bfloat16))
    lower = (grad - upper.astype(jnp.float32)).astype(jnp.bfloat16)

    gate_cot = gate_cotangent(log_cache, cache_cot, ends, me)
    gate_part = jnp.dot(gate_cot, saved_input, preferred_element_type=jnp.float32)

    def projected(pieces):
        pieces = jnp.moveaxis(pieces, 0, 1).reshape(roles, peers * rows, half)
        return sum(
            jnp.einsum("rdk,rdw->rkw", pieces, side, preferred_element_type=jnp.float32)
            for side in (upper, lower)
        )

    parts = jnp.concatenate(
        [
            projected(near).reshape(-1, width),
            projected(far).reshape(-1, width),
            gate_part.reshape(-1, width),
        ]
    )
    lines = parts.shape[0]
    arrived = lax.all_to_all(
        parts.reshape(peers, lines // peers, width), FS, split_axis=0, concat_axis=0, tiled=True
    )
    sums = from_everyone(jnp.sum(arrived, axis=0)[None], FS).reshape(lines, width)
    pair = sums[: roles * rank].reshape(cores, roles, half, width)
    low = jnp.where(core == 0, pair, pair[::-1])
    low = jnp.moveaxis(low, 0, 1).reshape(roles, rank, width)
    gate_grad = sums[roles * rank :].reshape(heads, -1)

    first_new = BETA_ONE * first_moment + (1.0 - BETA_ONE) * low
    second_new = BETA_TWO * second_moment + (1.0 - BETA_TWO) * low * low
    direction = first_new / jnp.sqrt(second_new)
    squares = jnp.sum(from_everyone(jnp.sum(direction * direction).reshape(1, 1), TP))
    entries = direction.size * lax.axis_size(TP)
    scale = lax.rsqrt(squares / entries + 1e-06)
    product = jnp.einsum(
        "rdk,rkw->rdw", factors.astype(jnp.float32), direction, precision=lax.Precision.HIGHEST
    )
    proj_step = scale * product
    proj_new = proj_master - LEARN * proj_step
    proj_copy = from_everyone(proj_new.astype(jnp.bfloat16)[None], FS)
    proj_copy = proj_copy.reshape(peers, roles, rows, width)
    proj_copy = jnp.moveaxis(proj_copy, 0, 1).reshape(roles, peers * rows, width)
    gate_first_new = BETA_ONE * gate_first + (1.0 - BETA_ONE) * gate_grad
    gate_second_new = BETA_TWO * gate_second + (1.0 - BETA_TWO) * gate_grad * gate_grad
    gate_new = gate_master - LEARN * gate_first_new / jnp.sqrt(gate_second_new)
    return (
        proj_step,
        proj_new,
        proj_copy,
        first_new,
        second_new,
        gate_new,
        gate_new.astype(jnp.bfloat16),
        gate_first_new,
        gate_second_new,
    )


def solution(mesh):
    fine = Mesh(mesh.devices.reshape(4, 4, 4, 2), (*FS, *TP))
    placed = (
        P(FS, None),
        P(None, FS, TP),
        P(None, FS),
        P(None, FS),
        P(None, FS, TP),
        P(None, FS, None),
        P(None, None, TP),
        P(None, None, TP),
        P(),
        P(),
        P(),
    )
    return jax.shard_map(
        local,
        mesh=fine,
        in_specs=placed,
        out_specs=(
            P(None, FS, TP),
            P(None, FS, TP),
            P(None, None, TP),
            P(None, None, TP),
            P(None, None, TP),
            P(),
            P(),
            P(),
            P(),
        ),
        check_vma=False,
    )
```

```python
import jax
import jax.numpy as jnp
from jax import lax
from jax.experimental import pallas as pl
from jax.experimental.pallas import tpu as pltpu
from jax.sharding import Mesh
from jax.sharding import PartitionSpec as P

BETA_ONE = 0.8
BETA_TWO = 0.9
LEARN = 0.001
FS = ("z", "x")
TP = ("y", "c")


def from_everyone(x, axis):
    copies = jnp.broadcast_to(x, (lax.axis_size(axis), *x.shape))
    return lax.all_to_all(copies, axis, split_axis=0, concat_axis=0, tiled=True)


VMEM = pl.BlockSpec(memory_space=pltpu.VMEM)
SMEM = pl.BlockSpec(memory_space=pltpu.SMEM)
ROOM = pltpu.CompilerParams(vmem_limit_bytes=48 * 2**20)


def cost(flops, moved):
    return pl.CostEstimate(flops=flops, bytes_accessed=moved, transcendentals=0)


def halves(x):
    upper = x.astype(jnp.bfloat16)
    return upper, (x - upper.astype(jnp.float32)).astype(jnp.bfloat16)


def pack_kernel(place_ref, factor_ref, log_ref, cot_ref, out_ref):
    peers, lines, lanes = out_ref.shape
    heads, length = log_ref.shape
    roles, rows, _ = factor_ref.shape
    column = lax.broadcasted_iota(jnp.int32, (heads, lanes), 1)
    row = lax.broadcasted_iota(jnp.int32, (heads, lanes), 0)
    ends = jnp.sum(jnp.where(column == row, jnp.sum(cot_ref[...], axis=1, keepdims=True), 0.0), axis=0, keepdims=True)
    last = log_ref[:, length - 1 :]
    ends = ends + jnp.sum(jnp.where(column == row + heads, last, 0.0), axis=0, keepdims=True)
    upper, lower = halves(ends)
    rest = ends - upper.astype(jnp.float32)
    rest = rest - lower.astype(jnp.float32)
    line = lax.broadcasted_iota(jnp.int32, (lines - roles * rows, lanes), 0)
    tail = jnp.where(line == 0, upper.astype(jnp.float32), 0.0)
    tail = jnp.where(line == 1, lower.astype(jnp.float32), tail)
    tail = jnp.where(line == 2, rest, tail).astype(jnp.bfloat16)
    for peer in range(peers):
        for role in range(roles):
            out_ref[peer, role * rows : (role + 1) * rows, :] = factor_ref[role]
        out_ref[peer, roles * rows :, :] = tail


def packed(place, factors, log_cache, cache_cot, peers):
    roles, rows, rank = factors.shape
    heads, length = log_cache.shape
    shape = (peers, roles * rows + 16, rank // 2)
    whole = lambda i, place: (0, 0)
    return pl.pallas_call(
        pack_kernel,
        out_shape=jax.ShapeDtypeStruct(shape, jnp.bfloat16),
        grid_spec=pltpu.PrefetchScalarGridSpec(
            num_scalar_prefetch=1,
            grid=(1,),
            in_specs=[
                pl.BlockSpec((roles, rows, rank // 2), lambda i, place: (0, 0, place[2])),
                pl.BlockSpec((heads, length), whole),
                pl.BlockSpec((heads, length), whole),
            ],
            out_specs=pl.BlockSpec(shape, lambda i, place: (0, 0, 0)),
        ),
        compiler_params=ROOM,
        cost_estimate=cost(10**6, 2 * 10**6),
        name="packed",
    )(place, factors, log_cache, cache_cot)


def gate_kernel(place_ref, log_ref, cot_ref, ends_ref, input_ref, out_ref):
    me = place_ref[0]
    heads, length = log_ref.shape
    ends = ends_ref[...].astype(jnp.float32)
    ends = ends[:, 0, :] + ends[:, 1, :] + ends[:, 2, :]
    source = lax.broadcasted_iota(jnp.int32, ends.shape, 0)
    after = jnp.sum(jnp.where(source > me, ends, 0.0), axis=0, keepdims=True)
    before = jnp.sum(jnp.where(source == me - 1, ends, 0.0), axis=0, keepdims=True)
    lane = lax.broadcasted_iota(jnp.int32, (heads, ends.shape[1]), 1)
    row = lax.broadcasted_iota(jnp.int32, (heads, ends.shape[1]), 0)
    carried = jnp.sum(jnp.where(lane == row, after, 0.0), axis=1, keepdims=True)
    edge = jnp.sum(jnp.where(lane == row + heads, before, 0.0), axis=1, keepdims=True)
    place = lax.broadcasted_iota(jnp.int32, (heads, length), 1)
    total = cot_ref[...]
    step = 1
    while step < length:
        total = total + jnp.where(place < length - step, pltpu.roll(total, length - step, 1), 0.0)
        step *= 2
    log = log_ref[...]
    previous = jnp.where(place == 0, edge, pltpu.roll(log, 1, 1))
    delta = log - previous
    closed = -jnp.tanh(0.5 * delta) * (jnp.exp(delta) + 1.0)
    gate_cot = ((total + carried) * closed).astype(jnp.bfloat16)
    out_ref[...] = jnp.dot(gate_cot, input_ref[...], preferred_element_type=jnp.float32)


def gate_columns(place, log_cache, cache_cot, ends, saved_input, width):
    heads, length = log_cache.shape
    peers, lines, lanes = ends.shape
    whole = lambda i, place: (0, 0)
    return pl.pallas_call(
        gate_kernel,
        out_shape=jax.ShapeDtypeStruct((heads, width), jnp.float32),
        grid_spec=pltpu.PrefetchScalarGridSpec(
            num_scalar_prefetch=1,
            grid=(1,),
            in_specs=[
                pl.BlockSpec((heads, length), whole),
                pl.BlockSpec((heads, length), whole),
                pl.BlockSpec((peers, 16, lanes), lambda i, place: (0, lines // 16 - 1, 0)),
                pl.BlockSpec((length, width), lambda i, place: (0, place[1])),
            ],
            out_specs=pl.BlockSpec((heads, width), whole),
        ),
        compiler_params=ROOM,
        cost_estimate=cost(4 * 10**9, 4 * 10**6),
        name="gate_columns",
    )(place, log_cache, cache_cot, ends, saved_input)


def low_kernel(grad_ref, near_ref, far_ref, out_ref):
    role = pl.program_id(0)
    peers, rows, half = near_ref.shape
    sides = [ref[...].reshape(peers * rows, half) for ref in (near_ref, far_ref)]
    pieces = jnp.concatenate(sides, axis=1)
    upper, lower = halves(grad_ref[0])
    low = jnp.dot(upper, pieces, preferred_element_type=jnp.float32)
    low = low + jnp.dot(lower, pieces, preferred_element_type=jnp.float32)
    low = low.T
    lines = half // peers
    for side in range(2):
        part = low[side * half : (side + 1) * half].reshape(peers, lines, -1)
        start = pl.multiple_of(side * 3 * lines + role * lines, lines)
        out_ref[:, pl.ds(start, lines), :] = part


def low_parts(grad, near, far):
    roles, width, depth = grad.shape
    peers, _, half = near.shape
    rows = depth // peers
    lines = 2 * roles * half // peers
    factor_spec = pl.BlockSpec((peers, rows, half), lambda r: (0, r, 0))
    return pl.pallas_call(
        low_kernel,
        out_shape=jax.ShapeDtypeStruct((peers, lines, width), jnp.float32),
        grid=(roles,),
        in_specs=[
            pl.BlockSpec((1, width, depth), lambda r: (r, 0, 0)),
            factor_spec,
            factor_spec,
        ],
        out_specs=pl.BlockSpec((peers, lines, width), lambda r: (0, 0, 0)),
        compiler_params=ROOM,
        cost_estimate=cost(4 * roles * width * depth * 2 * half, 11 * 10**6),
        name="low_parts",
    )(grad, near, far)


def sum_kernel(arrived_ref, gate_ref, out_ref):
    peers, lines, _ = arrived_ref.shape
    total = jnp.sum(arrived_ref[...], axis=0)
    gate = gate_ref[...]
    for peer in range(peers):
        out_ref[peer, :lines, :] = total
        out_ref[peer, lines:, :] = gate


def summed(arrived, gate):
    peers, lines, width = arrived.shape
    return pl.pallas_call(
        sum_kernel,
        out_shape=jax.ShapeDtypeStruct((peers, lines + gate.shape[0], width), jnp.float32),
        in_specs=[VMEM, VMEM],
        out_specs=VMEM,
        compiler_params=ROOM,
        cost_estimate=cost(10**6, 2 * 10**6),
        name="summed",
    )(arrived, gate)


def moment_kernel(
    place_ref, sums_ref, first_ref, second_ref, first_new_ref, second_new_ref, upper_ref,
    lower_ref, shared_ref,
):
    core = place_ref[2]
    roles, rank, width = first_ref.shape
    peers, _, _ = sums_ref.shape
    half = rank // 2
    block = half // peers
    squares = jnp.zeros((half, width), jnp.float32)
    for side in range(2):
        for role in range(roles):
            at = (side * roles + role) * block
            low = sums_ref[:, at : at + block, :].reshape(half, width)
            at = pl.ds(pl.multiple_of((core ^ side) * half, half), half)
            first_new = BETA_ONE * first_ref[role, at] + (1.0 - BETA_ONE) * low
            second_new = BETA_TWO * second_ref[role, at] + (1.0 - BETA_TWO) * low * low
            direction = first_new / jnp.sqrt(second_new)
            first_new_ref[role, at] = first_new
            second_new_ref[role, at] = second_new
            squares = squares + direction * direction
            upper_ref[role, at], lower_ref[role, at] = halves(direction)
    squares = jnp.sum(squares, axis=(0, 1), keepdims=True)
    gate = jnp.sum(sums_ref[:, 2 * roles * block :, :], axis=0)
    heads = gate.shape[0]
    for copy in range(shared_ref.shape[0]):
        shared_ref[copy, :heads, :] = gate
        shared_ref[copy, heads:, :] = jnp.broadcast_to(squares, (8, width))


def moments(place, sums, first_moment, second_moment, copies):
    shape = first_moment.shape
    heads = sums.shape[1] - 2 * shape[0] * (shape[1] // 2 // sums.shape[0])
    like = lambda dtype: jax.ShapeDtypeStruct(shape, dtype)
    return pl.pallas_call(
        moment_kernel,
        out_shape=[
            like(jnp.float32),
            like(jnp.float32),
            like(jnp.bfloat16),
            like(jnp.bfloat16),
            jax.ShapeDtypeStruct((copies, heads + 8, shape[2]), jnp.float32),
        ],
        in_specs=[SMEM, VMEM, VMEM, VMEM],
        out_specs=[VMEM] * 5,
        compiler_params=ROOM,
        cost_estimate=cost(10**7, 6 * 10**6),
        name="moments",
    )(place, sums, first_moment, second_moment)


def product_kernel(factor_ref, upper_ref, lower_ref, out_ref):
    for role in range(factor_ref.shape[0]):
        out_ref[role] = jnp.dot(
            factor_ref[role], upper_ref[role], preferred_element_type=jnp.float32
        ) + jnp.dot(factor_ref[role], lower_ref[role], preferred_element_type=jnp.float32)


def products(factors, upper, lower):
    roles, rows, rank = factors.shape
    width = upper.shape[2]
    return pl.pallas_call(
        product_kernel,
        out_shape=jax.ShapeDtypeStruct((roles, rows, width), jnp.float32),
        in_specs=[VMEM] * 3,
        out_specs=VMEM,
        compiler_params=ROOM,
        cost_estimate=cost(4 * roles * rows * rank * width, 2 * 10**6),
        name="products",
    )(factors, upper, lower)


def local(
    saved_input,
    proj_cot,
    log_cache,
    cache_cot,
    proj_master,
    factors,
    first_moment,
    second_moment,
    gate_master,
    gate_first,
    gate_second,
):
    roles, rows, _ = factors.shape
    heads = log_cache.shape[0]
    width = proj_cot.shape[2]
    peers = lax.axis_size(FS)
    core = lax.axis_index("c")
    place = jnp.stack([lax.axis_index(FS), lax.axis_index(TP), core]).astype(jnp.int32)

    near = packed(place, factors, log_cache, cache_cot, peers)
    near = lax.all_to_all(near, FS, split_axis=0, concat_axis=0, tiled=True)
    far = lax.ppermute(near, "c", [(0, 1), (1, 0)])
    grad = jnp.einsum("td,rtw->rwd", saved_input, proj_cot, preferred_element_type=jnp.float32)
    parts = low_parts(grad, near, far)
    arrived = lax.all_to_all(parts, FS, split_axis=0, concat_axis=0, tiled=True)
    gate_part = gate_columns(place, log_cache, cache_cot, near, saved_input, width)
    sums = lax.all_to_all(summed(arrived, gate_part), FS, split_axis=0, concat_axis=0, tiled=True)

    first_new, second_new, upper, lower, shared = moments(
        place, sums, first_moment, second_moment, lax.axis_size(TP)
    )
    shared = lax.all_to_all(shared, TP, split_axis=0, concat_axis=0, tiled=True)
    squares = jnp.sum(shared[:, heads, 0])
    entries = first_new.size * lax.axis_size(TP)
    scale = lax.rsqrt(squares / entries + 1e-06)
    product = products(factors, upper, lower)
    proj_step = scale * product
    proj_new = proj_master - LEARN * proj_step
    proj_copy = from_everyone(proj_new.astype(jnp.bfloat16)[None], FS)
    proj_copy = proj_copy.reshape(peers, roles, rows, width)
    proj_copy = jnp.moveaxis(proj_copy, 0, 1).reshape(roles, peers * rows, width)
    gate_grad = jnp.moveaxis(shared[:, :heads], 0, 1).reshape(heads, -1)
    gate_first_new = BETA_ONE * gate_first + (1.0 - BETA_ONE) * gate_grad
    gate_second_new = BETA_TWO * gate_second + (1.0 - BETA_TWO) * gate_grad * gate_grad
    gate_new = gate_master - LEARN * gate_first_new / jnp.sqrt(gate_second_new)
    return (
        proj_step,
        proj_new,
        proj_copy,
        first_new,
        second_new,
        gate_new,
        gate_new.astype(jnp.bfloat16),
        gate_first_new,
        gate_second_new,
    )


def solution(mesh):
    fine = Mesh(mesh.devices.reshape(4, 4, 4, 2), (*FS, *TP))
    placed = (
        P(FS, None),
        P(None, FS, TP),
        P(None, FS),
        P(None, FS),
        P(None, FS, TP),
        P(None, FS, None),
        P(None, None, TP),
        P(None, None, TP),
        P(),
        P(),
        P(),
    )

    return jax.shard_map(
        local,
        mesh=fine,
        in_specs=placed,
        out_specs=(
            P(None, FS, TP),
            P(None, FS, TP),
            P(None, None, TP),
            P(None, None, TP),
            P(None, None, TP),
            P(),
            P(),
            P(),
            P(),
        ),
        check_vma=False,
    )
```

```python
import functools

import jax
import jax.numpy as jnp
from jax import lax
from jax.experimental import pallas as pl
from jax.experimental.pallas import tpu as pltpu
from jax.sharding import Mesh
from jax.sharding import PartitionSpec as P

BETA_ONE = 0.8
BETA_TWO = 0.9
LEARN = 0.001
FS = ("z", "x")
TP = ("y", "c")


VMEM = pl.BlockSpec(memory_space=pltpu.VMEM)
SMEM = pl.BlockSpec(memory_space=pltpu.SMEM)
HBM = pl.BlockSpec(memory_space=pltpu.HBM)


def room(mebibytes):
    return pltpu.CompilerParams(vmem_limit_bytes=mebibytes * 2**20)


def held(space, *arrays):
    return [pltpu.with_memory_space_constraint(a, space) for a in arrays]


def cost(flops, moved):
    return pl.CostEstimate(flops=flops, bytes_accessed=moved, transcendentals=0)


def halves(x):
    upper = x.astype(jnp.bfloat16)
    return upper, (x - upper.astype(jnp.float32)).astype(jnp.bfloat16)


def started(pairs, sems):
    copies = [pltpu.make_async_copy(a, b, sems.at[n]) for n, (a, b) in enumerate(pairs)]
    for copy in copies:
        copy.start()
    return copies


def finished(copies):
    for copy in copies:
        copy.wait()


def pack_kernel(
    place_ref, factor_ref, log_ref, cot_ref, out_ref, last, cot, block, read_sems, write_sems
):
    peers, lines, lanes = out_ref.shape
    heads, length = log_ref.shape
    roles, rows, _ = factor_ref.shape
    at = pl.ds(pl.multiple_of(place_ref[2] * lanes, lanes), lanes)
    reads = [(factor_ref.at[r, :, at], block.at[pl.ds(r * rows, rows)]) for r in range(roles)]
    reads += [(log_ref.at[:, pl.ds(length - lanes, lanes)], last), (cot_ref, cot)]
    finished(started(reads, read_sems))
    column = lax.broadcasted_iota(jnp.int32, (heads, lanes), 1)
    row = lax.broadcasted_iota(jnp.int32, (heads, lanes), 0)
    totals = jnp.sum(cot[...], axis=1, keepdims=True)
    ends = jnp.where(column == row, totals, 0.0)
    ends = ends + jnp.where(column == row + heads, last[:, lanes - 1 :], 0.0)
    ends = jnp.sum(ends, axis=0, keepdims=True)
    upper, lower = halves(ends)
    rest = ends - upper.astype(jnp.float32)
    rest = rest - lower.astype(jnp.float32)
    line = lax.broadcasted_iota(jnp.int32, (lines - roles * rows, lanes), 0)
    tail = jnp.where(line == 0, upper.astype(jnp.float32), 0.0)
    tail = jnp.where(line == 1, lower.astype(jnp.float32), tail)
    tail = jnp.where(line == 2, rest, tail).astype(jnp.bfloat16)
    block[roles * rows :, :] = tail
    finished(started([(block, out_ref.at[peer]) for peer in range(peers)], write_sems))


def packed(place, factors, log_cache, cache_cot, peers):
    roles, rows, rank = factors.shape
    heads, length = log_cache.shape
    lanes = rank // 2
    lines = roles * rows + 16
    return pl.pallas_call(
        pack_kernel,
        out_shape=pltpu.HBM((peers, lines, lanes), jnp.bfloat16),
        in_specs=[SMEM, HBM, HBM, HBM],
        out_specs=HBM,
        scratch_shapes=[
            pltpu.VMEM((heads, lanes), jnp.float32),
            pltpu.VMEM((heads, length), jnp.float32),
            pltpu.VMEM((lines, lanes), jnp.bfloat16),
            pltpu.SemaphoreType.DMA((roles + 2,)),
            pltpu.SemaphoreType.DMA((peers,)),
        ],
        compiler_params=room(8),
        cost_estimate=cost(10**6, 2 * 10**6),
        name="packed",
    )(place, *held(pltpu.HBM, factors, log_cache, cache_cot))


def gate_kernel(
    place_ref, log_hbm, cot_hbm, ends_hbm, input_hbm, out_ref, log_ref, cot_ref, ends_ref,
    input_ref, sems,
):
    lines, width = ends_hbm.shape[1], input_ref.shape[1]
    at = pl.ds(pl.multiple_of(place_ref[1] * width, width), width)
    reads = [
        (log_hbm, log_ref),
        (cot_hbm, cot_ref),
        (ends_hbm.at[:, pl.ds(lines - 16, 16)], ends_ref),
        (input_hbm.at[:, at], input_ref),
    ]
    reads = started(reads, sems)
    finished(reads[:3])
    me = place_ref[0]
    heads, length = log_ref.shape
    ends = ends_ref[...].astype(jnp.float32)
    ends = ends[:, 0, :] + ends[:, 1, :] + ends[:, 2, :]
    source = lax.broadcasted_iota(jnp.int32, ends.shape, 0)
    after = jnp.sum(jnp.where(source > me, ends, 0.0), axis=0, keepdims=True)
    before = jnp.sum(jnp.where(source == me - 1, ends, 0.0), axis=0, keepdims=True)
    lane = lax.broadcasted_iota(jnp.int32, (heads, ends.shape[1]), 1)
    row = lax.broadcasted_iota(jnp.int32, (heads, ends.shape[1]), 0)
    carried = jnp.sum(jnp.where(lane == row, after, 0.0), axis=1, keepdims=True)
    edge = jnp.sum(jnp.where(lane == row + heads, before, 0.0), axis=1, keepdims=True)
    place = lax.broadcasted_iota(jnp.int32, (heads, length), 1)
    total = cot_ref[...]
    step = 1
    while step < length:
        total = total + jnp.where(place < length - step, pltpu.roll(total, length - step, 1), 0.0)
        step *= 2
    log = log_ref[...]
    previous = jnp.where(place == 0, edge, pltpu.roll(log, 1, 1))
    delta = log - previous
    closed = -jnp.tanh(0.5 * delta) * (jnp.exp(delta) + 1.0)
    gate_cot = ((total + carried) * closed).astype(jnp.bfloat16)
    finished(reads[3:])
    out_ref[...] = jnp.dot(gate_cot, input_ref[...], preferred_element_type=jnp.float32)


def gate_columns(place, log_cache, cache_cot, ends, saved_input, width):
    heads, length = log_cache.shape
    peers, _, lanes = ends.shape
    return pl.pallas_call(
        gate_kernel,
        out_shape=jax.ShapeDtypeStruct((heads, width), jnp.float32),
        in_specs=[SMEM, HBM, HBM, HBM, HBM],
        out_specs=VMEM,
        scratch_shapes=[
            pltpu.VMEM((heads, length), jnp.float32),
            pltpu.VMEM((heads, length), jnp.float32),
            pltpu.VMEM((peers, 16, lanes), jnp.bfloat16),
            pltpu.VMEM((length, width), jnp.bfloat16),
            pltpu.SemaphoreType.DMA((4,)),
        ],
        compiler_params=room(10),
        cost_estimate=cost(4 * 10**9, 4 * 10**6),
        name="gate_columns",
    )(place, *held(pltpu.HBM, log_cache, cache_cot, ends, saved_input))


def low_kernel(grad_ref, near_ref, far_ref, out_ref):
    role = pl.program_id(0)
    peers, rows, half = near_ref.shape
    sides = [ref[...].reshape(peers * rows, half) for ref in (near_ref, far_ref)]
    pieces = jnp.concatenate(sides, axis=1)
    upper, lower = halves(grad_ref[0])
    low = jnp.dot(upper, pieces, preferred_element_type=jnp.float32)
    low = low + jnp.dot(lower, pieces, preferred_element_type=jnp.float32)
    low = low.T
    lines = half // peers
    for side in range(2):
        part = low[side * half : (side + 1) * half].reshape(peers, lines, -1)
        start = pl.multiple_of(side * 3 * lines + role * lines, lines)
        out_ref[:, pl.ds(start, lines), :] = part


def low_parts(grad, near, far):
    roles, width, depth = grad.shape
    peers, _, half = near.shape
    rows = depth // peers
    lines = 2 * roles * half // peers
    factor_spec = pl.BlockSpec((peers, rows, half), lambda r: (0, r, 0))
    return pl.pallas_call(
        low_kernel,
        out_shape=pltpu.HBM((peers, lines, width), jnp.float32),
        grid=(roles,),
        in_specs=[
            pl.BlockSpec((1, width, depth), lambda r: (r, 0, 0)),
            factor_spec,
            factor_spec,
        ],
        out_specs=pl.BlockSpec((peers, lines, width), lambda r: (0, 0, 0)),
        compiler_params=room(20),
        cost_estimate=cost(4 * roles * width * depth * 2 * half, 11 * 10**6),
        name="low_parts",
    )(*held(pltpu.HBM, grad), near, far)


def sum_kernel(arrived_ref, gate_ref, out_ref, block, sems):
    peers, lines, _ = arrived_ref.shape
    block[:lines, :] = jnp.sum(arrived_ref[...], axis=0)
    block[lines:, :] = gate_ref[...]
    finished(started([(block, out_ref.at[peer]) for peer in range(peers)], sems))


def summed(arrived, gate):
    peers, lines, width = arrived.shape
    lines = lines + gate.shape[0]
    return pl.pallas_call(
        sum_kernel,
        out_shape=pltpu.HBM((peers, lines, width), jnp.float32),
        in_specs=[VMEM, VMEM],
        out_specs=HBM,
        scratch_shapes=[
            pltpu.VMEM((lines, width), jnp.float32),
            pltpu.SemaphoreType.DMA((peers,)),
        ],
        compiler_params=room(8),
        cost_estimate=cost(10**6, 2 * 10**6),
        name="summed",
    )(arrived, gate)


def moment_kernel(
    place_ref, sums_ref, first_hbm, second_hbm, first_new_hbm, second_new_hbm, upper_ref,
    lower_ref, shared_hbm, first_ref, second_ref, first_new_ref, second_new_ref, message, sems,
):
    core = place_ref[2]
    finished(started([(first_hbm, first_ref), (second_hbm, second_ref)], sems))
    roles, rank, width = first_ref.shape
    peers, _, _ = sums_ref.shape
    half = rank // 2
    block = half // peers
    squares = jnp.zeros((half, width), jnp.float32)
    for side in range(2):
        for role in range(roles):
            at = (side * roles + role) * block
            low = sums_ref[:, at : at + block, :].reshape(half, width)
            at = pl.ds(pl.multiple_of((core ^ side) * half, half), half)
            first_new = BETA_ONE * first_ref[role, at] + (1.0 - BETA_ONE) * low
            second_new = BETA_TWO * second_ref[role, at] + (1.0 - BETA_TWO) * low * low
            direction = first_new / jnp.sqrt(second_new)
            first_new_ref[role, at] = first_new
            second_new_ref[role, at] = second_new
            squares = squares + direction * direction
            upper_ref[role, at], lower_ref[role, at] = halves(direction)
    squares = jnp.sum(squares, axis=(0, 1), keepdims=True)
    gate = jnp.sum(sums_ref[:, 2 * roles * block :, :], axis=0)
    heads = gate.shape[0]
    message[:heads, :] = gate
    message[heads:, :] = jnp.broadcast_to(squares, (8, width))
    writes = [(message, shared_hbm.at[copy]) for copy in range(shared_hbm.shape[0])]
    writes += [(first_new_ref, first_new_hbm), (second_new_ref, second_new_hbm)]
    finished(started(writes, sems))


def moments(place, sums, first_moment, second_moment, copies):
    shape = first_moment.shape
    heads = sums.shape[1] - 2 * shape[0] * (shape[1] // 2 // sums.shape[0])
    return pl.pallas_call(
        moment_kernel,
        out_shape=[
            pltpu.HBM(shape, jnp.float32),
            pltpu.HBM(shape, jnp.float32),
            pltpu.VMEM(shape, jnp.bfloat16),
            pltpu.VMEM(shape, jnp.bfloat16),
            pltpu.HBM((copies, heads + 8, shape[2]), jnp.float32),
        ],
        in_specs=[SMEM, VMEM, HBM, HBM],
        out_specs=[HBM, HBM, VMEM, VMEM, HBM],
        scratch_shapes=[pltpu.VMEM(shape, jnp.float32)] * 4
        + [
            pltpu.VMEM((heads + 8, shape[2]), jnp.float32),
            pltpu.SemaphoreType.DMA((copies + 2,)),
        ],
        compiler_params=room(12),
        cost_estimate=cost(10**7, 6 * 10**6),
        name="moments",
    )(place, sums, *held(pltpu.HBM, first_moment, second_moment))


def product_kernel(place_ref, near_ref, far_ref, upper_ref, lower_ref, out_ref):
    roles, depth, _ = out_ref.shape
    peers, _, half = near_ref.shape
    rows = depth // peers
    core = place_ref[2]
    for role in range(roles):
        total = None
        for side, ref in enumerate((near_ref, far_ref)):
            pieces = ref[:, role * rows : (role + 1) * rows, :].reshape(depth, half)
            at = pl.ds(pl.multiple_of((core ^ side) * half, half), half)
            for part in (upper_ref, lower_ref):
                term = jnp.dot(pieces, part[role, at], preferred_element_type=jnp.float32)
                total = term if total is None else total + term
        out_ref[role] = total


def products(place, near, far, upper, lower, rows):
    roles, rank, width = upper.shape
    depth = near.shape[0] * rows
    return pl.pallas_call(
        product_kernel,
        out_shape=pltpu.VMEM((roles, depth, width), jnp.float32),
        in_specs=[SMEM, VMEM, VMEM, VMEM, VMEM],
        out_specs=VMEM,
        compiler_params=room(20),
        cost_estimate=cost(4 * roles * depth * rank * width, 10**7),
        name="products",
    )(place, near, far, *held(pltpu.VMEM, upper, lower))


def final_kernel(entries, place_ref, shared_ref, product_ref, *refs):
    pieces, refs = refs[:10], refs[10:]
    inputs, outputs, refs = refs[:4], refs[4:11], refs[11:]
    kept, made, read_sems, write_sems = refs[:4], refs[4:11], refs[11], refs[12]
    master_ref, gate_master_ref, gate_first_ref, gate_second_ref = kept
    step_ref, new_ref, copy_ref, *gate_refs = made
    reads = started(zip(inputs, kept), read_sems)
    heads = gate_master_ref.shape[0]
    roles, rows, width = master_ref.shape
    squares = jnp.sum(shared_ref[:, heads, 0:1], axis=0, keepdims=True)
    scale = 1.0 / jnp.sqrt(squares / entries + 1e-06)
    along = place_ref[3], place_ref[4]
    side = rows // 2
    writes = []
    for role in range(roles):
        for part in range(2):
            for first in range(4):
                for second in range(4):
                    offsets = (first, second) if part == 0 else (second, first)
                    source = [(along[n] + 4 - offsets[n]) % 4 for n in range(2)]
                    source = source[0] * 4 + source[1]
                    if second == 2:
                        ref, index = pieces[part * 5 + 3 + first // 2], first % 2
                    else:
                        ref, index = pieces[part * 5 + (0, 1, None, 2)[second]], first
                    at = pl.ds(pl.multiple_of(source * rows + part * side, side), side)
                    step = scale * product_ref[role, at]
                    new = ref[index, role] - LEARN * step
                    copy_ref[role, at] = new.astype(jnp.bfloat16)
        writes += started([(copy_ref.at[role], outputs[2].at[role])], write_sems.at[pl.ds(role, 1)])
    finished(reads)
    at = pl.ds(pl.multiple_of(place_ref[0] * rows, rows), rows)
    for role in range(roles):
        step = scale * product_ref[role, at]
        step_ref[role] = step
        new_ref[role] = master_ref[role] - LEARN * step
    for peer in range(shared_ref.shape[0]):
        at = slice(peer * width, (peer + 1) * width)
        grad = shared_ref[peer, :heads]
        first = BETA_ONE * gate_first_ref[:, at] + (1.0 - BETA_ONE) * grad
        second = BETA_TWO * gate_second_ref[:, at] + (1.0 - BETA_TWO) * grad * grad
        new = gate_master_ref[:, at] - LEARN * first / jnp.sqrt(second)
        gate_refs[0][:, at] = new
        gate_refs[1][:, at] = new.astype(jnp.bfloat16)
        gate_refs[2][:, at] = first
        gate_refs[3][:, at] = second
    rest = [(made[n], outputs[n]) for n in (0, 1, 3, 4, 5, 6)]
    finished(writes + started(rest, write_sems.at[pl.ds(roles, 6)]))


def finals(entries, place, shared, product, pieces, master, gates):
    roles = master.shape[0]
    outs = [
        (master.shape, jnp.float32),
        (master.shape, jnp.float32),
        (product.shape, jnp.bfloat16),
        (gates[0].shape, jnp.float32),
        (gates[0].shape, jnp.bfloat16),
        (gates[0].shape, jnp.float32),
        (gates[0].shape, jnp.float32),
    ]
    kept = [(a.shape, a.dtype) for a in (master, *gates)]
    return pl.pallas_call(
        functools.partial(final_kernel, entries),
        out_shape=[pltpu.HBM(*out) for out in outs],
        in_specs=[SMEM, VMEM, VMEM] + [VMEM] * 10 + [HBM] * 4,
        out_specs=[HBM] * 7,
        scratch_shapes=[pltpu.VMEM(*a) for a in kept + outs]
        + [pltpu.SemaphoreType.DMA((4,)), pltpu.SemaphoreType.DMA((roles + 6,))],
        compiler_params=room(20),
        cost_estimate=cost(10**7, 16 * 10**6),
        name="finals",
    )(place, shared, *held(pltpu.VMEM, product), *pieces, *held(pltpu.HBM, master, *gates))


def shift(x, axis, by):
    return lax.ppermute(x, axis, [(i, (i + by) % 4) for i in range(4)])


def local(
    saved_input,
    proj_cot,
    log_cache,
    cache_cot,
    proj_master,
    factors,
    first_moment,
    second_moment,
    gate_master,
    gate_first,
    gate_second,
):
    roles, rows, _ = factors.shape
    width = proj_cot.shape[2]
    peers = lax.axis_size(FS)
    place = [lax.axis_index(name) for name in (FS, TP, "c", "z", "x")]
    place = jnp.stack(place).astype(jnp.int32)

    near = packed(place, factors, log_cache, cache_cot, peers)
    near = lax.all_to_all(near, FS, split_axis=0, concat_axis=0, tiled=True)
    far = lax.ppermute(near, "c", [(0, 1), (1, 0)])
    sides = proj_master.reshape(roles, 2, rows // 2, width)
    sides = [(sides[:, part][None], axis) for part, axis in enumerate(FS)]
    sides = [[side] + [shift(side, axis, by) for by in (1, 2, 3)] for side, axis in sides]
    sides = [jnp.concatenate(side) for side in sides]
    ahead = [shift(side, axis, 1) for side, axis in zip(sides, FS[::-1])]
    behind = [shift(side, axis, 3) for side, axis in zip(sides, FS[::-1])]
    opposite = [shift(side[:2], axis, 1) for side, axis in zip(ahead, FS[::-1])]
    other = [shift(side[2:], axis, 3) for side, axis in zip(behind, FS[::-1])]
    pieces = [x for group in zip(sides, ahead, behind, opposite, other) for x in group]
    grad = jnp.einsum("td,rtw->rwd", saved_input, proj_cot, preferred_element_type=jnp.float32)
    parts = low_parts(grad, near, far)
    arrived = lax.all_to_all(parts, FS, split_axis=0, concat_axis=0, tiled=True)
    gate_part = gate_columns(place, log_cache, cache_cot, near, saved_input, width)
    sums = lax.all_to_all(summed(arrived, gate_part), FS, split_axis=0, concat_axis=0, tiled=True)

    first_new, second_new, upper, lower, shared = moments(
        place, sums, first_moment, second_moment, lax.axis_size(TP)
    )
    shared = lax.all_to_all(shared, TP, split_axis=0, concat_axis=0, tiled=True)
    product = products(place, near, far, upper, lower, rows)
    entries = first_new.size * lax.axis_size(TP)
    gates = (gate_master, gate_first, gate_second)
    step, new, copy, *gates = finals(entries, place, shared, product, pieces, proj_master, gates)
    return step, new, copy, first_new, second_new, *gates


def solution(mesh):
    fine = Mesh(mesh.devices.reshape(4, 4, 4, 2), (*FS, *TP))
    placed = (
        P(FS, None),
        P(None, FS, TP),
        P(None, FS),
        P(None, FS),
        P(None, FS, TP),
        P(None, FS, None),
        P(None, None, TP),
        P(None, None, TP),
        P(),
        P(),
        P(),
    )

    return jax.shard_map(
        local,
        mesh=fine,
        in_specs=placed,
        out_specs=(
            P(None, FS, TP),
            P(None, FS, TP),
            P(None, None, TP),
            P(None, None, TP),
            P(None, None, TP),
            P(),
            P(),
            P(),
            P(),
        ),
        check_vma=False,
    )
```

```python
import functools

import jax
import jax.numpy as jnp
from jax import lax
from jax.experimental import pallas as pl
from jax.experimental.pallas import tpu as pltpu
from jax.sharding import Mesh
from jax.sharding import PartitionSpec as P

BETA_ONE = 0.8
BETA_TWO = 0.9
LEARN = 0.001
FS = ("z", "x")
TP = ("y", "c")


VMEM = pl.BlockSpec(memory_space=pltpu.VMEM)
SMEM = pl.BlockSpec(memory_space=pltpu.SMEM)
HBM = pl.BlockSpec(memory_space=pltpu.HBM)


def room(mebibytes):
    return pltpu.CompilerParams(vmem_limit_bytes=mebibytes * 2**20)


def held(space, *arrays):
    return [pltpu.with_memory_space_constraint(a, space) for a in arrays]


def cost(flops, moved):
    return pl.CostEstimate(flops=flops, bytes_accessed=moved, transcendentals=0)


def halves(x):
    upper = x.astype(jnp.bfloat16)
    return upper, (x - upper.astype(jnp.float32)).astype(jnp.bfloat16)


def started(pairs, sems):
    copies = [pltpu.make_async_copy(a, b, sems.at[n]) for n, (a, b) in enumerate(pairs)]
    for copy in copies:
        copy.start()
    return copies


def finished(copies):
    for copy in copies:
        copy.wait()


def pack_kernel(
    place_ref, factor_ref, log_ref, cot_ref, out_ref, last, cot, block, read_sems, write_sems
):
    peers, lines, lanes = out_ref.shape
    heads, length = log_ref.shape
    roles, rows, _ = factor_ref.shape
    at = pl.ds(pl.multiple_of(place_ref[2] * lanes, lanes), lanes)
    reads = [(factor_ref.at[r, :, at], block.at[pl.ds(r * rows, rows)]) for r in range(roles)]
    reads += [(log_ref.at[:, pl.ds(length - lanes, lanes)], last), (cot_ref, cot)]
    finished(started(reads, read_sems))
    column = lax.broadcasted_iota(jnp.int32, (heads, lanes), 1)
    row = lax.broadcasted_iota(jnp.int32, (heads, lanes), 0)
    totals = jnp.sum(cot[...], axis=1, keepdims=True)
    ends = jnp.where(column == row, totals, 0.0)
    ends = ends + jnp.where(column == row + heads, last[:, lanes - 1 :], 0.0)
    ends = jnp.sum(ends, axis=0, keepdims=True)
    upper, lower = halves(ends)
    rest = ends - upper.astype(jnp.float32)
    rest = rest - lower.astype(jnp.float32)
    line = lax.broadcasted_iota(jnp.int32, (lines - roles * rows, lanes), 0)
    tail = jnp.where(line == 0, upper.astype(jnp.float32), 0.0)
    tail = jnp.where(line == 1, lower.astype(jnp.float32), tail)
    tail = jnp.where(line == 2, rest, tail).astype(jnp.bfloat16)
    block[roles * rows :, :] = tail
    finished(started([(block, out_ref.at[peer]) for peer in range(peers)], write_sems))


def packed(place, factors, log_cache, cache_cot, peers):
    roles, rows, rank = factors.shape
    heads, length = log_cache.shape
    lanes = rank // 2
    lines = roles * rows + 16
    return pl.pallas_call(
        pack_kernel,
        out_shape=pltpu.HBM((peers, lines, lanes), jnp.bfloat16),
        in_specs=[SMEM, HBM, HBM, HBM],
        out_specs=HBM,
        scratch_shapes=[
            pltpu.VMEM((heads, lanes), jnp.float32),
            pltpu.VMEM((heads, length), jnp.float32),
            pltpu.VMEM((lines, lanes), jnp.bfloat16),
            pltpu.SemaphoreType.DMA((roles + 2,)),
            pltpu.SemaphoreType.DMA((peers,)),
        ],
        compiler_params=room(8),
        cost_estimate=cost(10**6, 2 * 10**6),
        name="packed",
    )(place, *held(pltpu.HBM, factors, log_cache, cache_cot))


def gate_kernel(
    place_ref, log_hbm, cot_hbm, ends_hbm, input_hbm, out_ref, log_ref, cot_ref, ends_ref,
    input_ref, sems,
):
    lines, width = ends_hbm.shape[1], input_ref.shape[1]
    at = pl.ds(pl.multiple_of(place_ref[1] * width, width), width)
    reads = [
        (log_hbm, log_ref),
        (cot_hbm, cot_ref),
        (ends_hbm.at[:, pl.ds(lines - 16, 16)], ends_ref),
        (input_hbm.at[:, at], input_ref),
    ]
    reads = started(reads, sems)
    finished(reads[:3])
    me = place_ref[0]
    heads, length = log_ref.shape
    ends = ends_ref[...].astype(jnp.float32)
    ends = ends[:, 0, :] + ends[:, 1, :] + ends[:, 2, :]
    source = lax.broadcasted_iota(jnp.int32, ends.shape, 0)
    after = jnp.sum(jnp.where(source > me, ends, 0.0), axis=0, keepdims=True)
    before = jnp.sum(jnp.where(source == me - 1, ends, 0.0), axis=0, keepdims=True)
    lane = lax.broadcasted_iota(jnp.int32, (heads, ends.shape[1]), 1)
    row = lax.broadcasted_iota(jnp.int32, (heads, ends.shape[1]), 0)
    carried = jnp.sum(jnp.where(lane == row, after, 0.0), axis=1, keepdims=True)
    edge = jnp.sum(jnp.where(lane == row + heads, before, 0.0), axis=1, keepdims=True)
    place = lax.broadcasted_iota(jnp.int32, (heads, length), 1)
    total = cot_ref[...]
    step = 1
    while step < length:
        total = total + jnp.where(place < length - step, pltpu.roll(total, length - step, 1), 0.0)
        step *= 2
    log = log_ref[...]
    previous = jnp.where(place == 0, edge, pltpu.roll(log, 1, 1))
    delta = log - previous
    closed = -jnp.tanh(0.5 * delta) * (jnp.exp(delta) + 1.0)
    gate_cot = ((total + carried) * closed).astype(jnp.bfloat16)
    finished(reads[3:])
    out_ref[...] = jnp.dot(gate_cot, input_ref[...], preferred_element_type=jnp.float32)


def gate_columns(place, log_cache, cache_cot, ends, saved_input, width):
    heads, length = log_cache.shape
    peers, _, lanes = ends.shape
    return pl.pallas_call(
        gate_kernel,
        out_shape=jax.ShapeDtypeStruct((heads, width), jnp.float32),
        in_specs=[SMEM, HBM, HBM, HBM, HBM],
        out_specs=VMEM,
        scratch_shapes=[
            pltpu.VMEM((heads, length), jnp.float32),
            pltpu.VMEM((heads, length), jnp.float32),
            pltpu.VMEM((peers, 16, lanes), jnp.bfloat16),
            pltpu.VMEM((length, width), jnp.bfloat16),
            pltpu.SemaphoreType.DMA((4,)),
        ],
        compiler_params=room(10),
        cost_estimate=cost(4 * 10**9, 4 * 10**6),
        name="gate_columns",
    )(place, *held(pltpu.HBM, log_cache, cache_cot, ends, saved_input))


def low_kernel(grad_ref, near_ref, far_ref, gate_ref, out_ref):
    role = pl.program_id(0)
    peers, rows, half = near_ref.shape
    sides = [ref[...].reshape(peers * rows, half) for ref in (near_ref, far_ref)]
    pieces = jnp.concatenate(sides, axis=1)
    upper, lower = halves(grad_ref[0])
    low = jnp.dot(upper, pieces, preferred_element_type=jnp.float32)
    low = low + jnp.dot(lower, pieces, preferred_element_type=jnp.float32)
    low = low.T
    lines = half // peers
    for side in range(2):
        part = low[side * half : (side + 1) * half].reshape(peers, lines, -1)
        start = pl.multiple_of(side * 3 * lines + role * lines, lines)
        out_ref[:, pl.ds(start, lines), :] = part

    @pl.when(role == 0)
    def _():
        out_ref[:, 6 * lines :, :] = jnp.zeros_like(out_ref[:, 6 * lines :, :])
        for head in range(gate_ref.shape[0]):
            out_ref[head, 6 * lines : 6 * lines + 1, :] = gate_ref[head : head + 1, :]


def low_parts(grad, near, far, gate):
    roles, width, depth = grad.shape
    peers, _, half = near.shape
    rows = depth // peers
    lines = 2 * roles * half // peers + 8
    factor_spec = pl.BlockSpec((peers, rows, half), lambda r: (0, r, 0))
    return pl.pallas_call(
        low_kernel,
        out_shape=pltpu.HBM((peers, lines, width), jnp.float32),
        grid=(roles,),
        in_specs=[
            pl.BlockSpec((1, width, depth), lambda r: (r, 0, 0)),
            factor_spec,
            factor_spec,
            pl.BlockSpec(gate.shape, lambda r: (0, 0)),
        ],
        out_specs=pl.BlockSpec((peers, lines, width), lambda r: (0, 0, 0)),
        compiler_params=room(20),
        cost_estimate=cost(4 * roles * width * depth * 2 * half, 11 * 10**6),
        name="low_parts",
    )(*held(pltpu.HBM, grad, near, far), gate)


def sum_kernel(arrived_ref, out_ref, block, sems):
    block[...] = jnp.sum(arrived_ref[...], axis=0)
    peers = out_ref.shape[0]
    finished(started([(block, out_ref.at[peer]) for peer in range(peers)], sems))


def summed(arrived):
    return pl.pallas_call(
        sum_kernel,
        out_shape=pltpu.HBM(arrived.shape, jnp.float32),
        in_specs=[VMEM],
        out_specs=HBM,
        scratch_shapes=[
            pltpu.VMEM(arrived.shape[1:], jnp.float32),
            pltpu.SemaphoreType.DMA((arrived.shape[0],)),
        ],
        compiler_params=room(8),
        cost_estimate=cost(10**6, 2 * 10**6),
        name="summed",
    )(arrived)


def moment_kernel(
    place_ref, sums_ref, first_hbm, second_hbm, first_new_hbm, second_new_hbm, upper_hbm,
    lower_hbm, shared_hbm, first_ref, second_ref, upper_ref, lower_ref, message, read_sems,
    write_sems,
):
    core = place_ref[2]
    roles, rank, width = first_ref.shape
    peers = sums_ref.shape[0]
    half = rank // 2
    block = half // peers
    reads = [
        started(
            [(first_hbm.at[role], first_ref.at[role]), (second_hbm.at[role], second_ref.at[role])],
            read_sems.at[role],
        )
        for role in range(roles)
    ]
    squares = jnp.zeros((half, width), jnp.float32)
    writes = []
    for role in range(roles):
        finished(reads[role])
        for side in range(2):
            at = (side * roles + role) * block
            low = sums_ref[:, at : at + block, :].reshape(half, width)
            at = pl.ds(pl.multiple_of((core ^ side) * half, half), half)
            first_new = BETA_ONE * first_ref[role, at] + (1.0 - BETA_ONE) * low
            second_new = BETA_TWO * second_ref[role, at] + (1.0 - BETA_TWO) * low * low
            direction = first_new / jnp.sqrt(second_new)
            first_ref[role, at] = first_new
            second_ref[role, at] = second_new
            squares = squares + direction * direction
            upper, lower = halves(direction)
            upper_ref[role, side * half : (side + 1) * half] = upper
            lower_ref[role, side * half : (side + 1) * half] = lower
        made = [first_ref, second_ref, upper_ref, lower_ref]
        kept = [first_new_hbm, second_new_hbm, upper_hbm, lower_hbm]
        pairs = [(a.at[role], b.at[role]) for a, b in zip(made, kept)]
        writes += started(pairs, write_sems.at[pl.ds(role * 4, 4)])
    squares = jnp.sum(squares, axis=(0, 1), keepdims=True)
    heads = peers
    for head in range(heads):
        message[head : head + 1, :] = sums_ref[head, 6 * block : 6 * block + 1, :]
    message[heads:, :] = jnp.broadcast_to(squares, (8, width))
    copies = shared_hbm.shape[0]
    pairs = [(message, shared_hbm.at[copy]) for copy in range(copies)]
    finished(writes + started(pairs, write_sems.at[pl.ds(roles * 4, copies)]))


def moments(place, sums, first_moment, second_moment, copies):
    shape = first_moment.shape
    heads = sums.shape[0]
    return pl.pallas_call(
        moment_kernel,
        out_shape=[
            pltpu.HBM(shape, jnp.float32),
            pltpu.HBM(shape, jnp.float32),
            pltpu.HBM(shape, jnp.bfloat16),
            pltpu.HBM(shape, jnp.bfloat16),
            pltpu.HBM((copies, heads + 8, shape[2]), jnp.float32),
        ],
        in_specs=[SMEM, VMEM, HBM, HBM],
        out_specs=[HBM] * 5,
        scratch_shapes=[pltpu.VMEM(shape, jnp.float32)] * 2
        + [pltpu.VMEM(shape, jnp.bfloat16)] * 2
        + [
            pltpu.VMEM((heads + 8, shape[2]), jnp.float32),
            pltpu.SemaphoreType.DMA((shape[0], 2)),
            pltpu.SemaphoreType.DMA((shape[0] * 4 + copies,)),
        ],
        compiler_params=room(12),
        cost_estimate=cost(10**7, 6 * 10**6),
        name="moments",
    )(place, sums, *held(pltpu.HBM, first_moment, second_moment))


def product_kernel(
    near_hbm, far_hbm, upper_hbm, lower_hbm, out_hbm, factor_ref, direction_ref, product_ref,
    read_sems, write_sems,
):
    roles, peers, rows, rank = factor_ref.shape
    half = rank // 2

    def operands(role):
        lines = pl.ds(role * rows, rows)
        pairs = [
            (ref.at[:, lines, :], factor_ref.at[role, :, :, pl.ds(side * half, half)])
            for side, ref in enumerate((near_hbm, far_hbm))
        ]
        directions = enumerate((upper_hbm, lower_hbm))
        pairs += [(ref.at[role], direction_ref.at[role, n]) for n, ref in directions]
        return started(pairs, read_sems.at[role])

    reads = [operands(role) for role in range(roles)]
    writes = []
    for role in range(roles):
        finished(reads[role])
        factor = factor_ref[role].reshape(peers * rows, rank)
        product_ref[role] = jnp.dot(
            factor, direction_ref[role, 0], preferred_element_type=jnp.float32
        ) + jnp.dot(factor, direction_ref[role, 1], preferred_element_type=jnp.float32)
        pairs = [(product_ref.at[role], out_hbm.at[role])]
        writes += started(pairs, write_sems.at[pl.ds(role, 1)])
    finished(writes)


def products(near, far, upper, lower, rows):
    roles, rank, width = upper.shape
    peers = near.shape[0]
    shape = (roles, peers * rows, width)
    return pl.pallas_call(
        product_kernel,
        out_shape=pltpu.HBM(shape, jnp.float32),
        in_specs=[HBM] * 4,
        out_specs=HBM,
        scratch_shapes=[
            pltpu.VMEM((roles, peers, rows, rank), jnp.bfloat16),
            pltpu.VMEM((roles, 2, rank, width), jnp.bfloat16),
            pltpu.VMEM(shape, jnp.float32),
            pltpu.SemaphoreType.DMA((roles, 4)),
            pltpu.SemaphoreType.DMA((roles,)),
        ],
        compiler_params=room(20),
        cost_estimate=cost(4 * roles * peers * rows * rank * width, 10**7),
        name="products",
    )(*held(pltpu.HBM, near, far, upper, lower))


def final_kernel(entries, place_ref, product_hbm, *refs):
    pieces, inputs, outputs, refs = refs[:18], refs[18:23], refs[23:30], refs[30:]
    product_ref, piece_refs, refs = refs[0], refs[1:19], refs[19:]
    kept, made, (piece_sems, rest_sems, write_sems) = refs[:5], refs[5:12], refs[12:]
    shared_ref, master_ref, gate_master_ref, gate_first_ref, gate_second_ref = kept
    step_ref, new_ref, copy_ref, *gate_refs = made
    heads = gate_master_ref.shape[0]
    roles, rows, width = master_ref.shape
    rest = started(zip(inputs, kept), rest_sems)
    waits = []
    for role in range(roles):
        pairs = [(product_hbm.at[role], product_ref.at[role])]
        chosen, index = (range(0, 5), role) if role + 1 < roles else (range(5, 9), 0)
        for n in [part * 9 + n for part in range(2) for n in chosen]:
            pairs.append((pieces[n].at[:, index], piece_refs[n].at[:, index]))
        waits.append(started(pairs, piece_sems.at[role]))
    along = place_ref[3], place_ref[4]
    side = rows // 2
    own = pl.ds(pl.multiple_of(place_ref[0] * rows, rows), rows)
    finished(rest)
    squares = jnp.sum(shared_ref[:, heads, 0:1], axis=0, keepdims=True)
    scale = 1.0 / jnp.sqrt(squares / entries + 1e-06)
    writes = []
    for peer in range(shared_ref.shape[0]):
        at = slice(peer * width, (peer + 1) * width)
        grad = shared_ref[peer, :heads]
        first = BETA_ONE * gate_first_ref[:, at] + (1.0 - BETA_ONE) * grad
        second = BETA_TWO * gate_second_ref[:, at] + (1.0 - BETA_TWO) * grad * grad
        new = gate_master_ref[:, at] - LEARN * first / jnp.sqrt(second)
        gate_refs[0][:, at] = new
        gate_refs[1][:, at] = new.astype(jnp.bfloat16)
        gate_refs[2][:, at] = first
        gate_refs[3][:, at] = second
    writes += started(zip(made[3:], outputs[3:]), write_sems.at[pl.ds(roles * 3, 4)])
    for role in range(roles):
        finished(waits[role])
        for part in range(2):
            for first in range(4):
                for second in range(4):
                    offsets = (first, second) if part == 0 else (second, first)
                    source = [(along[n] + 4 - offsets[n]) % 4 for n in range(2)]
                    source = source[0] * 4 + source[1]
                    at = pl.ds(pl.multiple_of(source * rows + part * side, side), side)
                    index = first
                    if role + 1 == roles:
                        ref = piece_refs[part * 9 + 5 + second][index, 0]
                    else:
                        place = (0, 1, 3 + first // 2, 2)[second]
                        index = first % 2 if second == 2 else first
                        ref = piece_refs[part * 9 + place][index, role]
                    new = ref - LEARN * (scale * product_ref[role, at])
                    copy_ref[role, at] = new.astype(jnp.bfloat16)
        step = scale * product_ref[role, own]
        step_ref[role] = step
        new_ref[role] = master_ref[role] - LEARN * step
        pairs = [(made[n].at[role], outputs[n].at[role]) for n in range(3)]
        writes += started(pairs, write_sems.at[pl.ds(role * 3, 3)])
    finished(writes)


def finals(entries, place, product, pieces, shared, master, gates):
    roles = master.shape[0]
    outs = [
        (master.shape, jnp.float32),
        (master.shape, jnp.float32),
        (product.shape, jnp.bfloat16),
        (gates[0].shape, jnp.float32),
        (gates[0].shape, jnp.bfloat16),
        (gates[0].shape, jnp.float32),
        (gates[0].shape, jnp.float32),
    ]
    inputs = (shared, master, *gates)
    kept = [(a.shape, a.dtype) for a in (product, *pieces, *inputs)]
    dma = pltpu.SemaphoreType.DMA
    return pl.pallas_call(
        functools.partial(final_kernel, entries),
        out_shape=[pltpu.HBM(*out) for out in outs],
        in_specs=[SMEM] + [HBM] * len(kept),
        out_specs=[HBM] * 7,
        scratch_shapes=[pltpu.VMEM(*a) for a in kept + outs]
        + [dma((roles, 11)), dma((5,)), dma((roles * 3 + 4,))],
        compiler_params=room(32),
        cost_estimate=cost(10**7, 16 * 10**6),
        name="finals",
    )(place, *held(pltpu.HBM, product, *pieces, *inputs))


def join_kernel(master_hbm, *refs):
    pieces, outs, blocks, (read_sems, write_sems) = refs[:6], refs[6:10], refs[10:12], refs[12:]
    early = outs[0].shape[1]
    side = master_hbm.shape[1] // 2
    pairs = []
    for part, block in enumerate(blocks):
        pairs.append((master_hbm.at[:, pl.ds(part * side, side)], block.at[0]))
        pairs += [(pieces[part * 3 + n].at[0], block.at[n + 1]) for n in range(3)]
    reads, writes = started(pairs, read_sems), []
    for n, read in enumerate(reads):
        read.wait()
        block = blocks[n // 4].at[n % 4]
        pairs = [
            (block.at[pl.ds(0, early)], outs[n // 4].at[n % 4]),
            (block.at[pl.ds(early, block.shape[0] - early)], outs[2 + n // 4].at[n % 4]),
        ]
        writes += started(pairs, write_sems.at[pl.ds(n * 2, 2)])
    finished(writes)


def joined(master, pieces, early):
    shape = (4, *pieces[0].shape[1:])
    return pl.pallas_call(
        join_kernel,
        out_shape=[
            pltpu.HBM((4, count, *shape[2:]), jnp.float32)
            for count in (early, early, shape[1] - early, shape[1] - early)
        ],
        in_specs=[HBM] * 7,
        out_specs=[HBM] * 4,
        scratch_shapes=[pltpu.VMEM(shape, jnp.float32)] * 2
        + [pltpu.SemaphoreType.DMA((8,)), pltpu.SemaphoreType.DMA((16,))],
        compiler_params=room(4),
        cost_estimate=cost(10**6, 6 * 10**6),
        name="joined",
    )(*held(pltpu.HBM, master, *pieces))


def shift(x, axis, by):
    return lax.ppermute(x, axis, [(i, (i + by) % 4) for i in range(4)])


def local(
    saved_input,
    proj_cot,
    log_cache,
    cache_cot,
    proj_master,
    factors,
    first_moment,
    second_moment,
    gate_master,
    gate_first,
    gate_second,
):
    roles, rows, _ = factors.shape
    width = proj_cot.shape[2]
    peers = lax.axis_size(FS)
    place = [lax.axis_index(name) for name in (FS, TP, "c", "z", "x")]
    place = jnp.stack(place).astype(jnp.int32)

    near = packed(place, factors, log_cache, cache_cot, peers)
    near = lax.all_to_all(near, FS, split_axis=0, concat_axis=0, tiled=True)
    far = lax.ppermute(near, "c", [(0, 1), (1, 0)])
    sides = proj_master.reshape(roles, 2, rows // 2, width)
    spread = [
        shift(sides[:, part][None], axis, by) for part, axis in enumerate(FS) for by in (1, 2, 3)
    ]
    axes = FS[::-1]
    *early, first_late, second_late = joined(proj_master, spread, roles - 1)
    late = (first_late, second_late)
    ahead = [shift(side, axis, 1) for side, axis in zip(early, axes)]
    behind = [shift(side, axis, 3) for side, axis in zip(early, axes)]
    opposite = [shift(side[:2], axis, 1) for side, axis in zip(ahead, axes)]
    other = [shift(side[2:], axis, 3) for side, axis in zip(behind, axes)]
    late = [[side] + [shift(side, axis, by) for by in (1, 2, 3)] for side, axis in zip(late, axes)]
    pieces = [
        [*group, *rest] for *group, rest in zip(early, ahead, behind, opposite, other, late)
    ]
    pieces = [piece for group in pieces for piece in group]
    grad = jnp.einsum("td,rtw->rwd", saved_input, proj_cot, preferred_element_type=jnp.float32)
    gate_part = gate_columns(place, log_cache, cache_cot, near, saved_input, width)
    parts = low_parts(grad, near, far, gate_part)
    arrived = lax.all_to_all(parts, FS, split_axis=0, concat_axis=0, tiled=True)
    sums = lax.all_to_all(summed(arrived), FS, split_axis=0, concat_axis=0, tiled=True)

    first_new, second_new, upper, lower, shared = moments(
        place, sums, first_moment, second_moment, lax.axis_size(TP)
    )
    shared = lax.all_to_all(shared, TP, split_axis=0, concat_axis=0, tiled=True)
    product = products(near, far, upper, lower, rows)
    entries = first_new.size * lax.axis_size(TP)
    gates = (gate_master, gate_first, gate_second)
    step, new, copy, *gates = finals(entries, place, product, pieces, shared, proj_master, gates)
    return step, new, copy, first_new, second_new, *gates


def solution(mesh):
    fine = Mesh(mesh.devices.reshape(4, 4, 4, 2), (*FS, *TP))
    placed = (
        P(FS, None),
        P(None, FS, TP),
        P(None, FS),
        P(None, FS),
        P(None, FS, TP),
        P(None, FS, None),
        P(None, None, TP),
        P(None, None, TP),
        P(),
        P(),
        P(),
    )

    return jax.shard_map(
        local,
        mesh=fine,
        in_specs=placed,
        out_specs=(
            P(None, FS, TP),
            P(None, FS, TP),
            P(None, None, TP),
            P(None, None, TP),
            P(None, None, TP),
            P(),
            P(),
            P(),
            P(),
        ),
        check_vma=False,
    )
```

```python
import functools

import jax
import jax.numpy as jnp
from jax import lax
from jax.experimental import pallas as pl
from jax.experimental.pallas import tpu as pltpu
from jax.sharding import Mesh
from jax.sharding import PartitionSpec as P

BETA_ONE = 0.8
BETA_TWO = 0.9
LEARN = 0.001
FS = ("z", "x")
NEXT = (1, 2, 10, 11)
TP = ("y", "c")


VMEM = pl.BlockSpec(memory_space=pltpu.VMEM)
SMEM = pl.BlockSpec(memory_space=pltpu.SMEM)
HBM = pl.BlockSpec(memory_space=pltpu.HBM)


def room(mebibytes):
    return pltpu.CompilerParams(vmem_limit_bytes=mebibytes * 2**20)


def held(space, *arrays):
    return [pltpu.with_memory_space_constraint(a, space) for a in arrays]


def cost(flops, moved):
    return pl.CostEstimate(flops=flops, bytes_accessed=moved, transcendentals=0)


def halves(x):
    upper = x.astype(jnp.bfloat16)
    return upper, (x - upper.astype(jnp.float32)).astype(jnp.bfloat16)


def started(pairs, sems):
    copies = [pltpu.make_async_copy(a, b, sems.at[n]) for n, (a, b) in enumerate(pairs)]
    for copy in copies:
        copy.start()
    return copies


def finished(copies):
    for copy in copies:
        copy.wait()


def pack_kernel(
    place_ref, factor_ref, log_ref, cot_ref, out_ref, last, cot, block, read_sems, write_sems
):
    peers, lines, lanes = out_ref.shape
    heads, length = log_ref.shape
    roles, rows, _ = factor_ref.shape
    at = pl.ds(pl.multiple_of(place_ref[2] * lanes, lanes), lanes)
    reads = [(factor_ref.at[r, :, at], block.at[pl.ds(r * rows, rows)]) for r in range(roles)]
    reads += [(log_ref.at[:, pl.ds(length - lanes, lanes)], last), (cot_ref, cot)]
    reads = started(reads, read_sems)
    finished(reads[:roles])
    body, rest_of = pl.ds(0, roles * rows), pl.ds(roles * rows, lines - roles * rows)
    pairs = [(block.at[body], out_ref.at[peer, body]) for peer in range(peers)]
    writes = started(pairs, write_sems.at[pl.ds(0, peers)])
    finished(reads[roles:])
    column = lax.broadcasted_iota(jnp.int32, (heads, lanes), 1)
    row = lax.broadcasted_iota(jnp.int32, (heads, lanes), 0)
    totals = jnp.sum(cot[...], axis=1, keepdims=True)
    ends = jnp.where(column == row, totals, 0.0)
    ends = ends + jnp.where(column == row + heads, last[:, lanes - 1 :], 0.0)
    ends = jnp.sum(ends, axis=0, keepdims=True)
    upper, lower = halves(ends)
    rest = ends - upper.astype(jnp.float32)
    rest = rest - lower.astype(jnp.float32)
    line = lax.broadcasted_iota(jnp.int32, (lines - roles * rows, lanes), 0)
    tail = jnp.where(line == 0, upper.astype(jnp.float32), 0.0)
    tail = jnp.where(line == 1, lower.astype(jnp.float32), tail)
    tail = jnp.where(line == 2, rest, tail).astype(jnp.bfloat16)
    block[roles * rows :, :] = tail
    pairs = [(block.at[rest_of], out_ref.at[peer, rest_of]) for peer in range(peers)]
    finished(writes + started(pairs, write_sems.at[pl.ds(peers, peers)]))


def packed(place, factors, log_cache, cache_cot, peers):
    roles, rows, rank = factors.shape
    heads, length = log_cache.shape
    lanes = rank // 2
    lines = roles * rows + 16
    return pl.pallas_call(
        pack_kernel,
        out_shape=pltpu.HBM((peers, lines, lanes), jnp.bfloat16),
        in_specs=[SMEM, HBM, HBM, HBM],
        out_specs=HBM,
        scratch_shapes=[
            pltpu.VMEM((heads, lanes), jnp.float32),
            pltpu.VMEM((heads, length), jnp.float32),
            pltpu.VMEM((lines, lanes), jnp.bfloat16),
            pltpu.SemaphoreType.DMA((roles + 2,)),
            pltpu.SemaphoreType.DMA((2 * peers,)),
        ],
        compiler_params=room(8),
        cost_estimate=cost(10**6, 2 * 10**6),
        name="packed",
    )(place, *held(pltpu.HBM, factors, log_cache, cache_cot))


def gate_kernel(
    place_ref, log_hbm, cot_hbm, ends_hbm, input_hbm, out_ref, log_ref, cot_ref, ends_ref,
    input_ref, sems,
):
    lines, width = ends_hbm.shape[1], input_ref.shape[1]
    at = pl.ds(pl.multiple_of(place_ref[1] * width, width), width)
    reads = [
        (log_hbm, log_ref),
        (cot_hbm, cot_ref),
        (ends_hbm.at[:, pl.ds(lines - 16, 16)], ends_ref),
        (input_hbm.at[:, at], input_ref),
    ]
    reads = started(reads, sems)
    finished(reads[:3])
    me = place_ref[0]
    heads, length = log_ref.shape
    ends = ends_ref[...].astype(jnp.float32)
    ends = ends[:, 0, :] + ends[:, 1, :] + ends[:, 2, :]
    source = lax.broadcasted_iota(jnp.int32, ends.shape, 0)
    after = jnp.sum(jnp.where(source > me, ends, 0.0), axis=0, keepdims=True)
    before = jnp.sum(jnp.where(source == me - 1, ends, 0.0), axis=0, keepdims=True)
    lane = lax.broadcasted_iota(jnp.int32, (heads, ends.shape[1]), 1)
    row = lax.broadcasted_iota(jnp.int32, (heads, ends.shape[1]), 0)
    carried = jnp.sum(jnp.where(lane == row, after, 0.0), axis=1, keepdims=True)
    edge = jnp.sum(jnp.where(lane == row + heads, before, 0.0), axis=1, keepdims=True)
    place = lax.broadcasted_iota(jnp.int32, (heads, length), 1)
    total = cot_ref[...]
    step = 1
    while step < length:
        total = total + jnp.where(place < length - step, pltpu.roll(total, length - step, 1), 0.0)
        step *= 2
    log = log_ref[...]
    previous = jnp.where(place == 0, edge, pltpu.roll(log, 1, 1))
    delta = log - previous
    closed = -jnp.tanh(0.5 * delta) * (jnp.exp(delta) + 1.0)
    gate_cot = ((total + carried) * closed).astype(jnp.bfloat16)
    finished(reads[3:])
    out_ref[...] = jnp.dot(gate_cot, input_ref[...], preferred_element_type=jnp.float32)


def gate_columns(place, log_cache, cache_cot, ends, saved_input, width):
    heads, length = log_cache.shape
    peers, _, lanes = ends.shape
    return pl.pallas_call(
        gate_kernel,
        out_shape=jax.ShapeDtypeStruct((heads, width), jnp.float32),
        in_specs=[SMEM, HBM, HBM, pl.BlockSpec(memory_space=pl.ANY), HBM],
        out_specs=VMEM,
        scratch_shapes=[
            pltpu.VMEM((heads, length), jnp.float32),
            pltpu.VMEM((heads, length), jnp.float32),
            pltpu.VMEM((peers, 16, lanes), jnp.bfloat16),
            pltpu.VMEM((length, width), jnp.bfloat16),
            pltpu.SemaphoreType.DMA((4,)),
        ],
        compiler_params=room(10),
        cost_estimate=cost(4 * 10**9, 4 * 10**6),
        name="gate_columns",
    )(place, *held(pltpu.HBM, log_cache, cache_cot), ends, *held(pltpu.HBM, saved_input))


def low_kernel(
    grad_hbm, near_ref, far_ref, gate_ref, out_hbm, grad_ref, out_ref, tail_ref, read_sems,
    write_sems,
):
    roles, width, depth = grad_ref.shape
    peers, _, half = near_ref.shape
    rows = depth // peers
    lines = half // peers
    pairs = [(grad_hbm.at[role], grad_ref.at[role]) for role in range(roles)]
    reads = started(pairs, read_sems)
    tail_ref[...] = jnp.zeros_like(tail_ref)
    for head in range(gate_ref.shape[0]):
        tail_ref[head, 0:1, :] = gate_ref[head : head + 1, :]
    writes = [(tail_ref, out_hbm.at[:, pl.ds(2 * roles * lines, tail_ref.shape[1])])]
    writes = started(writes, write_sems.at[pl.ds(2 * roles, 1)])
    for role in range(roles):
        at = slice(role * rows, (role + 1) * rows)
        sides = [ref[:, at, :].reshape(depth, half) for ref in (near_ref, far_ref)]
        pieces = jnp.concatenate(sides, axis=1)
        reads[role].wait()
        both = jnp.concatenate(halves(grad_ref[role]), axis=0)
        low = jnp.dot(both, pieces, preferred_element_type=jnp.float32)
        low = (low[:width] + low[width:]).T
        pairs = []
        for side in range(2):
            part = low[side * half : (side + 1) * half].reshape(peers, lines, width)
            out_ref[side, role] = part
            place = pl.ds((side * roles + role) * lines, lines)
            pairs.append((out_ref.at[side, role], out_hbm.at[:, place]))
        writes += started(pairs, write_sems.at[pl.ds(2 * role, 2)])
    finished(writes)


def low_parts(grad, near, far, gate):
    roles, width, depth = grad.shape
    peers, _, half = near.shape
    lines = half // peers
    return pl.pallas_call(
        low_kernel,
        out_shape=pltpu.HBM((peers, 2 * roles * lines + 8, width), jnp.float32),
        in_specs=[HBM, VMEM, VMEM, VMEM],
        out_specs=HBM,
        scratch_shapes=[
            pltpu.VMEM(grad.shape, jnp.float32),
            pltpu.VMEM((2, roles, peers, lines, width), jnp.float32),
            pltpu.VMEM((peers, 8, width), jnp.float32),
            pltpu.SemaphoreType.DMA((roles,)),
            pltpu.SemaphoreType.DMA((2 * roles + 1,)),
        ],
        compiler_params=room(22),
        cost_estimate=cost(4 * roles * width * depth * 2 * half, 11 * 10**6),
        name="low_parts",
    )(*held(pltpu.HBM, grad), near, far, gate)


def sum_kernel(arrived_ref, out_ref, block, sems):
    block[...] = jnp.sum(arrived_ref[...], axis=0)
    peers = out_ref.shape[0]
    finished(started([(block, out_ref.at[peer]) for peer in range(peers)], sems))


def summed(arrived):
    return pl.pallas_call(
        sum_kernel,
        out_shape=pltpu.HBM(arrived.shape, jnp.float32),
        in_specs=[VMEM],
        out_specs=HBM,
        scratch_shapes=[
            pltpu.VMEM(arrived.shape[1:], jnp.float32),
            pltpu.SemaphoreType.DMA((arrived.shape[0],)),
        ],
        compiler_params=room(8),
        cost_estimate=cost(10**6, 2 * 10**6),
        name="summed",
    )(arrived)


def moment_kernel(
    place_ref, sums_ref, first_hbm, second_hbm, first_new_hbm, second_new_hbm, upper_hbm,
    lower_hbm, shared_hbm, first_ref, second_ref, upper_ref, lower_ref, message, read_sems,
    write_sems,
):
    core = place_ref[2]
    roles, rank, width = first_ref.shape
    peers = sums_ref.shape[0]
    half = rank // 2
    block = half // peers
    reads = [
        started(
            [(first_hbm.at[role], first_ref.at[role]), (second_hbm.at[role], second_ref.at[role])],
            read_sems.at[role],
        )
        for role in range(roles)
    ]
    squares = jnp.zeros((half, width), jnp.float32)
    writes = []
    for role in range(roles):
        finished(reads[role])
        for side in range(2):
            at = (side * roles + role) * block
            low = sums_ref[:, at : at + block, :].reshape(half, width)
            at = pl.ds(pl.multiple_of((core ^ side) * half, half), half)
            first_new = BETA_ONE * first_ref[role, at] + (1.0 - BETA_ONE) * low
            second_new = BETA_TWO * second_ref[role, at] + (1.0 - BETA_TWO) * low * low
            direction = first_new / jnp.sqrt(second_new)
            first_ref[role, at] = first_new
            second_ref[role, at] = second_new
            squares = squares + direction * direction
            upper, lower = halves(direction)
            upper_ref[role, side * half : (side + 1) * half] = upper
            lower_ref[role, side * half : (side + 1) * half] = lower
        made = [first_ref, second_ref, upper_ref, lower_ref]
        kept = [first_new_hbm, second_new_hbm, upper_hbm, lower_hbm]
        pairs = [(a.at[role], b.at[role]) for a, b in zip(made, kept)]
        writes += started(pairs, write_sems.at[pl.ds(role * 4, 4)])
    squares = jnp.sum(squares, axis=(0, 1), keepdims=True)
    heads = peers
    for head in range(heads):
        message[head : head + 1, :] = sums_ref[head, 6 * block : 6 * block + 1, :]
    message[heads:, :] = jnp.broadcast_to(squares, (8, width))
    copies = shared_hbm.shape[0]
    pairs = [(message, shared_hbm.at[copy]) for copy in range(copies)]
    finished(writes + started(pairs, write_sems.at[pl.ds(roles * 4, copies)]))


def moments(place, sums, first_moment, second_moment, copies):
    shape = first_moment.shape
    heads = sums.shape[0]
    return pl.pallas_call(
        moment_kernel,
        out_shape=[
            pltpu.HBM(shape, jnp.float32),
            pltpu.HBM(shape, jnp.float32),
            pltpu.HBM(shape, jnp.bfloat16),
            pltpu.HBM(shape, jnp.bfloat16),
            pltpu.HBM((copies, heads + 8, shape[2]), jnp.float32),
        ],
        in_specs=[SMEM, VMEM, HBM, HBM],
        out_specs=[HBM] * 5,
        scratch_shapes=[pltpu.VMEM(shape, jnp.float32)] * 2
        + [pltpu.VMEM(shape, jnp.bfloat16)] * 2
        + [
            pltpu.VMEM((heads + 8, shape[2]), jnp.float32),
            pltpu.SemaphoreType.DMA((shape[0], 2)),
            pltpu.SemaphoreType.DMA((shape[0] * 4 + copies,)),
        ],
        compiler_params=room(12),
        cost_estimate=cost(10**7, 6 * 10**6),
        name="moments",
    )(place, sums, *held(pltpu.HBM, first_moment, second_moment))


def product_kernel(
    near_hbm, far_hbm, upper_hbm, lower_hbm, out_hbm, factor_ref, direction_ref, product_ref,
    read_sems, write_sems,
):
    roles, peers, rows, rank = factor_ref.shape
    half = rank // 2

    def operands(role):
        lines = pl.ds(role * rows, rows)
        pairs = [
            (ref.at[:, lines, :], factor_ref.at[role, :, :, pl.ds(side * half, half)])
            for side, ref in enumerate((near_hbm, far_hbm))
        ]
        directions = enumerate((upper_hbm, lower_hbm))
        pairs += [(ref.at[role], direction_ref.at[role, n]) for n, ref in directions]
        return started(pairs, read_sems.at[role])

    reads = [operands(role) for role in range(roles)]
    writes = []
    for role in range(roles):
        finished(reads[role])
        factor = factor_ref[role].reshape(peers * rows, rank)
        product_ref[role] = jnp.dot(
            factor, direction_ref[role, 0], preferred_element_type=jnp.float32
        ) + jnp.dot(factor, direction_ref[role, 1], preferred_element_type=jnp.float32)
        pairs = [(product_ref.at[role], out_hbm.at[role])]
        writes += started(pairs, write_sems.at[pl.ds(role, 1)])
    finished(writes)


def products(near, far, upper, lower, rows):
    roles, rank, width = upper.shape
    peers = near.shape[0]
    shape = (roles, peers * rows, width)
    return pl.pallas_call(
        product_kernel,
        out_shape=pltpu.HBM(shape, jnp.float32),
        in_specs=[HBM] * 4,
        out_specs=HBM,
        scratch_shapes=[
            pltpu.VMEM((roles, peers, rows, rank), jnp.bfloat16),
            pltpu.VMEM((roles, 2, rank, width), jnp.bfloat16),
            pltpu.VMEM(shape, jnp.float32),
            pltpu.SemaphoreType.DMA((roles, 4)),
            pltpu.SemaphoreType.DMA((roles,)),
        ],
        compiler_params=room(20),
        cost_estimate=cost(4 * roles * peers * rows * rank * width, 10**7),
        name="products",
    )(*held(pltpu.HBM, near, far, upper, lower))


def final_kernel(entries, place_ref, product_hbm, *refs):
    pieces, shared_ref, inputs, outputs, refs = refs[:18], refs[18], refs[19:23], refs[23:30], refs[30:]
    count = 18 - len(NEXT)
    product_ref, piece_refs, refs = refs[0], list(refs[1 : count + 1]), refs[count + 1 :]
    kept, made, (piece_sems, rest_sems, write_sems) = refs[:4], refs[4:11], refs[11:]
    for n in NEXT:
        piece_refs.insert(n, pieces[n])
    master_ref, gate_master_ref, gate_first_ref, gate_second_ref = kept
    step_ref, new_ref, copy_ref, *gate_refs = made
    heads = gate_master_ref.shape[0]
    roles, rows, width = master_ref.shape
    rest = started(zip(inputs, kept), rest_sems)
    waits = []
    for role in range(roles):
        pairs = [(product_hbm.at[role], product_ref.at[role])]
        chosen, index = (range(0, 5), role) if role + 1 < roles else (range(5, 9), 0)
        for n in [part * 9 + n for part in range(2) for n in chosen if part * 9 + n not in NEXT]:
            pairs.append((pieces[n].at[:, index], piece_refs[n].at[:, index]))
        waits.append(started(pairs, piece_sems.at[role]))
    along = place_ref[3], place_ref[4]
    side = rows // 2
    own = pl.ds(pl.multiple_of(place_ref[0] * rows, rows), rows)
    finished(rest)
    squares = jnp.sum(shared_ref[:, heads, 0:1], axis=0, keepdims=True)
    scale = 1.0 / jnp.sqrt(squares / entries + 1e-06)
    writes = []
    for peer in range(shared_ref.shape[0]):
        at = slice(peer * width, (peer + 1) * width)
        grad = shared_ref[peer, :heads]
        first = BETA_ONE * gate_first_ref[:, at] + (1.0 - BETA_ONE) * grad
        second = BETA_TWO * gate_second_ref[:, at] + (1.0 - BETA_TWO) * grad * grad
        new = gate_master_ref[:, at] - LEARN * first / jnp.sqrt(second)
        gate_refs[0][:, at] = new
        gate_refs[1][:, at] = new.astype(jnp.bfloat16)
        gate_refs[2][:, at] = first
        gate_refs[3][:, at] = second
    writes += started(zip(made[3:], outputs[3:]), write_sems.at[pl.ds(roles * 3, 4)])
    for role in range(roles):
        finished(waits[role])
        for part in range(2):
            for first in range(4):
                for second in range(4):
                    offsets = (first, second) if part == 0 else (second, first)
                    source = [(along[n] + 4 - offsets[n]) % 4 for n in range(2)]
                    source = source[0] * 4 + source[1]
                    at = pl.ds(pl.multiple_of(source * rows + part * side, side), side)
                    index = first
                    if role + 1 == roles:
                        ref = piece_refs[part * 9 + 5 + second][index, 0]
                    else:
                        place = (0, 1, 3 + first // 2, 2)[second]
                        index = first % 2 if second == 2 else first
                        ref = piece_refs[part * 9 + place][index, role]
                    new = ref - LEARN * (scale * product_ref[role, at])
                    copy_ref[role, at] = new.astype(jnp.bfloat16)
        step = scale * product_ref[role, own]
        step_ref[role] = step
        new_ref[role] = master_ref[role] - LEARN * step
        pairs = [(made[n].at[role], outputs[n].at[role]) for n in range(3)]
        writes += started(pairs, write_sems.at[pl.ds(role * 3, 3)])
    finished(writes)


def finals(entries, place, product, pieces, shared, master, gates):
    roles = master.shape[0]
    outs = [
        (master.shape, jnp.float32),
        (master.shape, jnp.float32),
        (product.shape, jnp.bfloat16),
        (gates[0].shape, jnp.float32),
        (gates[0].shape, jnp.bfloat16),
        (gates[0].shape, jnp.float32),
        (gates[0].shape, jnp.float32),
    ]
    inputs = (master, *gates)
    copied = [piece for n, piece in enumerate(pieces) if n not in NEXT]
    kept = [(a.shape, a.dtype) for a in (product, *copied, *inputs)]
    pieces = [a if n in NEXT else held(pltpu.HBM, a)[0] for n, a in enumerate(pieces)]
    specs = [VMEM if n in NEXT else HBM for n in range(len(pieces))]
    dma = pltpu.SemaphoreType.DMA
    return pl.pallas_call(
        functools.partial(final_kernel, entries),
        out_shape=[pltpu.HBM(*out) for out in outs],
        in_specs=[SMEM, HBM, *specs, VMEM] + [HBM] * len(inputs),
        out_specs=[HBM] * 7,
        scratch_shapes=[pltpu.VMEM(*a) for a in kept + outs]
        + [dma((roles, 11)), dma((4,)), dma((roles * 3 + 4,))],
        compiler_params=room(32),
        cost_estimate=cost(10**7, 16 * 10**6),
        name="finals",
    )(place, *held(pltpu.HBM, product), *pieces, shared, *held(pltpu.HBM, *inputs))


def join_kernel(master_hbm, *refs):
    pieces, outs, blocks, (read_sems, write_sems) = refs[:6], refs[6:10], refs[10:12], refs[12:]
    early = outs[0].shape[1]
    side = master_hbm.shape[1] // 2
    pairs = []
    for part, block in enumerate(blocks):
        pairs.append((master_hbm.at[:, pl.ds(part * side, side)], block.at[0]))
        pairs += [(pieces[part * 3 + n].at[0], block.at[n + 1]) for n in range(3)]
    reads, writes = started(pairs, read_sems), []
    for n, read in enumerate(reads):
        read.wait()
        block = blocks[n // 4].at[n % 4]
        pairs = [
            (block.at[pl.ds(0, early)], outs[n // 4].at[n % 4]),
            (block.at[pl.ds(early, block.shape[0] - early)], outs[2 + n // 4].at[n % 4]),
        ]
        writes += started(pairs, write_sems.at[pl.ds(n * 2, 2)])
    finished(writes)


def joined(master, pieces, early):
    shape = (4, *pieces[0].shape[1:])
    return pl.pallas_call(
        join_kernel,
        out_shape=[
            pltpu.HBM((4, count, *shape[2:]), jnp.float32)
            for count in (early, early, shape[1] - early, shape[1] - early)
        ],
        in_specs=[HBM] * 7,
        out_specs=[HBM] * 4,
        scratch_shapes=[pltpu.VMEM(shape, jnp.float32)] * 2
        + [pltpu.SemaphoreType.DMA((8,)), pltpu.SemaphoreType.DMA((16,))],
        compiler_params=room(4),
        cost_estimate=cost(10**6, 6 * 10**6),
        name="joined",
    )(*held(pltpu.HBM, master, *pieces))


def shift(x, axis, by):
    return lax.ppermute(x, axis, [(i, (i + by) % 4) for i in range(4)])


def local(
    saved_input,
    proj_cot,
    log_cache,
    cache_cot,
    proj_master,
    factors,
    first_moment,
    second_moment,
    gate_master,
    gate_first,
    gate_second,
):
    roles, rows, _ = factors.shape
    width = proj_cot.shape[2]
    peers = lax.axis_size(FS)
    place = [lax.axis_index(name) for name in (FS, TP, "c", "z", "x")]
    place = jnp.stack(place).astype(jnp.int32)

    near = packed(place, factors, log_cache, cache_cot, peers)
    near = lax.all_to_all(near, FS, split_axis=0, concat_axis=0, tiled=True)
    far = lax.ppermute(near, "c", [(0, 1), (1, 0)])
    sides = proj_master.reshape(roles, 2, rows // 2, width)
    spread = [
        shift(sides[:, part][None], axis, by) for part, axis in enumerate(FS) for by in (1, 2, 3)
    ]
    axes = FS[::-1]
    *early, first_late, second_late = joined(proj_master, spread, roles - 1)
    late = (first_late, second_late)
    ahead = [shift(side, axis, 1) for side, axis in zip(early, axes)]
    behind = [shift(side, axis, 3) for side, axis in zip(early, axes)]
    opposite = [side[:2] for side in ahead]
    other = [side[2:] for side in behind]
    opposite = [shift(side, axis, 1) for side, axis in zip(opposite, axes)]
    other = [shift(side, axis, 3) for side, axis in zip(other, axes)]
    late = [[side] + [shift(side, axis, by) for by in (1, 2, 3)] for side, axis in zip(late, axes)]
    pieces = [
        [*group, *rest] for *group, rest in zip(early, ahead, behind, opposite, other, late)
    ]
    pieces = [piece for group in pieces for piece in group]
    grad = jnp.einsum("td,rtw->rwd", saved_input, proj_cot, preferred_element_type=jnp.float32)
    gate_part = gate_columns(place, log_cache, cache_cot, near, saved_input, width)
    parts = low_parts(grad, near, far, gate_part)
    arrived = lax.all_to_all(parts, FS, split_axis=0, concat_axis=0, tiled=True)
    sums = lax.all_to_all(summed(arrived), FS, split_axis=0, concat_axis=0, tiled=True)

    first_new, second_new, upper, lower, shared = moments(
        place, sums, first_moment, second_moment, lax.axis_size(TP)
    )
    shared = lax.all_to_all(shared, TP, split_axis=0, concat_axis=0, tiled=True)
    product = products(near, far, upper, lower, rows)
    entries = first_new.size * lax.axis_size(TP)
    gates = (gate_master, gate_first, gate_second)
    step, new, copy, *gates = finals(entries, place, product, pieces, shared, proj_master, gates)
    return step, new, copy, first_new, second_new, *gates


def solution(mesh):
    fine = Mesh(mesh.devices.reshape(4, 4, 4, 2), (*FS, *TP))
    placed = (
        P(FS, None),
        P(None, FS, TP),
        P(None, FS),
        P(None, FS),
        P(None, FS, TP),
        P(None, FS, None),
        P(None, None, TP),
        P(None, None, TP),
        P(),
        P(),
        P(),
    )

    return jax.shard_map(
        local,
        mesh=fine,
        in_specs=placed,
        out_specs=(
            P(None, FS, TP),
            P(None, FS, TP),
            P(None, None, TP),
            P(None, None, TP),
            P(None, None, TP),
            P(),
            P(),
            P(),
            P(),
        ),
        check_vma=False,
    )
```

```python
import functools

import jax
import jax.numpy as jnp
from jax import lax
from jax.experimental import pallas as pl
from jax.experimental.pallas import tpu as pltpu
from jax.sharding import Mesh
from jax.sharding import PartitionSpec as P

BETA_ONE = 0.8
BETA_TWO = 0.9
LEARN = 0.001
FS = ("z", "x")
NEXT = (1, 2, 10, 11)
TP = ("y", "c")


VMEM = pl.BlockSpec(memory_space=pltpu.VMEM)
SMEM = pl.BlockSpec(memory_space=pltpu.SMEM)
HBM = pl.BlockSpec(memory_space=pltpu.HBM)


def room(mebibytes):
    return pltpu.CompilerParams(vmem_limit_bytes=mebibytes * 2**20)


def held(space, *arrays):
    return [pltpu.with_memory_space_constraint(a, space) for a in arrays]


def cost(flops, moved):
    return pl.CostEstimate(flops=flops, bytes_accessed=moved, transcendentals=0)


def halves(x):
    upper = x.astype(jnp.bfloat16)
    return upper, (x - upper.astype(jnp.float32)).astype(jnp.bfloat16)


def started(pairs, sems):
    copies = [pltpu.make_async_copy(a, b, sems.at[n]) for n, (a, b) in enumerate(pairs)]
    for copy in copies:
        copy.start()
    return copies


def finished(copies):
    for copy in copies:
        copy.wait()


def pack_kernel(
    place_ref, factor_ref, log_ref, cot_ref, out_ref, last, cot, block, read_sems, write_sems
):
    peers, lines, lanes = out_ref.shape
    heads, length = log_ref.shape
    roles, rows, _ = factor_ref.shape
    at = pl.ds(pl.multiple_of(place_ref[2] * lanes, lanes), lanes)
    reads = [(factor_ref.at[r, :, at], block.at[pl.ds(r * rows, rows)]) for r in range(roles)]
    reads += [(log_ref.at[:, pl.ds(length - lanes, lanes)], last), (cot_ref, cot)]
    reads = started(reads, read_sems)
    finished(reads[:roles])
    body, rest_of = pl.ds(0, roles * rows), pl.ds(roles * rows, lines - roles * rows)
    pairs = [(block.at[body], out_ref.at[peer, body]) for peer in range(peers)]
    writes = started(pairs, write_sems.at[pl.ds(0, peers)])
    finished(reads[roles:])
    column = lax.broadcasted_iota(jnp.int32, (heads, lanes), 1)
    row = lax.broadcasted_iota(jnp.int32, (heads, lanes), 0)
    totals = jnp.sum(cot[...], axis=1, keepdims=True)
    ends = jnp.where(column == row, totals, 0.0)
    ends = ends + jnp.where(column == row + heads, last[:, lanes - 1 :], 0.0)
    ends = jnp.sum(ends, axis=0, keepdims=True)
    upper, lower = halves(ends)
    rest = ends - upper.astype(jnp.float32)
    rest = rest - lower.astype(jnp.float32)
    line = lax.broadcasted_iota(jnp.int32, (lines - roles * rows, lanes), 0)
    tail = jnp.where(line == 0, upper.astype(jnp.float32), 0.0)
    tail = jnp.where(line == 1, lower.astype(jnp.float32), tail)
    tail = jnp.where(line == 2, rest, tail).astype(jnp.bfloat16)
    block[roles * rows :, :] = tail
    pairs = [(block.at[rest_of], out_ref.at[peer, rest_of]) for peer in range(peers)]
    finished(writes + started(pairs, write_sems.at[pl.ds(peers, peers)]))


def packed(place, factors, log_cache, cache_cot, peers):
    roles, rows, rank = factors.shape
    heads, length = log_cache.shape
    lanes = rank // 2
    lines = roles * rows + 16
    return pl.pallas_call(
        pack_kernel,
        out_shape=pltpu.HBM((peers, lines, lanes), jnp.bfloat16),
        in_specs=[SMEM, HBM, HBM, HBM],
        out_specs=HBM,
        scratch_shapes=[
            pltpu.VMEM((heads, lanes), jnp.float32),
            pltpu.VMEM((heads, length), jnp.float32),
            pltpu.VMEM((lines, lanes), jnp.bfloat16),
            pltpu.SemaphoreType.DMA((roles + 2,)),
            pltpu.SemaphoreType.DMA((2 * peers,)),
        ],
        compiler_params=room(8),
        cost_estimate=cost(10**6, 2 * 10**6),
        name="packed",
    )(place, *held(pltpu.HBM, factors, log_cache, cache_cot))


def gate_kernel(
    place_ref, log_hbm, cot_hbm, ends_hbm, input_hbm, out_ref, log_ref, cot_ref, ends_ref,
    input_ref, sems,
):
    lines, width = ends_hbm.shape[1], input_ref.shape[1]
    at = pl.ds(pl.multiple_of(place_ref[1] * width, width), width)
    reads = [
        (log_hbm, log_ref),
        (cot_hbm, cot_ref),
        (ends_hbm.at[:, pl.ds(lines - 16, 16)], ends_ref),
        (input_hbm.at[:, at], input_ref),
    ]
    reads = started(reads, sems)
    finished(reads[:3])
    me = place_ref[0]
    heads, length = log_ref.shape
    ends = ends_ref[...].astype(jnp.float32)
    ends = ends[:, 0, :] + ends[:, 1, :] + ends[:, 2, :]
    source = lax.broadcasted_iota(jnp.int32, ends.shape, 0)
    after = jnp.sum(jnp.where(source > me, ends, 0.0), axis=0, keepdims=True)
    before = jnp.sum(jnp.where(source == me - 1, ends, 0.0), axis=0, keepdims=True)
    lane = lax.broadcasted_iota(jnp.int32, (heads, ends.shape[1]), 1)
    row = lax.broadcasted_iota(jnp.int32, (heads, ends.shape[1]), 0)
    carried = jnp.sum(jnp.where(lane == row, after, 0.0), axis=1, keepdims=True)
    edge = jnp.sum(jnp.where(lane == row + heads, before, 0.0), axis=1, keepdims=True)
    place = lax.broadcasted_iota(jnp.int32, (heads, length), 1)
    total = cot_ref[...]
    step = 1
    while step < length:
        total = total + jnp.where(place < length - step, pltpu.roll(total, length - step, 1), 0.0)
        step *= 2
    log = log_ref[...]
    previous = jnp.where(place == 0, edge, pltpu.roll(log, 1, 1))
    delta = log - previous
    closed = -jnp.tanh(0.5 * delta) * (jnp.exp(delta) + 1.0)
    gate_cot = ((total + carried) * closed).astype(jnp.bfloat16)
    finished(reads[3:])
    out_ref[...] = jnp.dot(gate_cot, input_ref[...], preferred_element_type=jnp.float32)


def gate_columns(place, log_cache, cache_cot, ends, saved_input, width):
    heads, length = log_cache.shape
    peers, _, lanes = ends.shape
    return pl.pallas_call(
        gate_kernel,
        out_shape=jax.ShapeDtypeStruct((heads, width), jnp.float32),
        in_specs=[SMEM, HBM, HBM, pl.BlockSpec(memory_space=pl.ANY), HBM],
        out_specs=VMEM,
        scratch_shapes=[
            pltpu.VMEM((heads, length), jnp.float32),
            pltpu.VMEM((heads, length), jnp.float32),
            pltpu.VMEM((peers, 16, lanes), jnp.bfloat16),
            pltpu.VMEM((length, width), jnp.bfloat16),
            pltpu.SemaphoreType.DMA((4,)),
        ],
        compiler_params=room(10),
        cost_estimate=cost(4 * 10**9, 4 * 10**6),
        name="gate_columns",
    )(place, *held(pltpu.HBM, log_cache, cache_cot), ends, *held(pltpu.HBM, saved_input))


def low_kernel(
    grad_ref, near_ref, far_ref, gate_ref, out_hbm, out_ref, tail_ref, write_sems,
):
    roles, width, depth = grad_ref.shape
    peers, _, half = near_ref.shape
    rows = depth // peers
    lines = half // peers
    tail_ref[...] = jnp.zeros_like(tail_ref)
    for head in range(gate_ref.shape[0]):
        tail_ref[head, 0:1, :] = gate_ref[head : head + 1, :]
    writes = [(tail_ref, out_hbm.at[:, pl.ds(2 * roles * lines, tail_ref.shape[1])])]
    writes = started(writes, write_sems.at[pl.ds(2 * roles, 1)])
    for role in range(roles):
        at = slice(role * rows, (role + 1) * rows)
        sides = [ref[:, at, :].reshape(depth, half) for ref in (near_ref, far_ref)]
        pieces = jnp.concatenate(sides, axis=1)
        both = jnp.concatenate(halves(grad_ref[role]), axis=0)
        low = jnp.dot(both, pieces, preferred_element_type=jnp.float32)
        low = (low[:width] + low[width:]).T
        pairs = []
        for side in range(2):
            part = low[side * half : (side + 1) * half].reshape(peers, lines, width)
            out_ref[side, role] = part
            place = pl.ds((side * roles + role) * lines, lines)
            pairs.append((out_ref.at[side, role], out_hbm.at[:, place]))
        writes += started(pairs, write_sems.at[pl.ds(2 * role, 2)])
    finished(writes)


def low_parts(grad, near, far, gate):
    roles, width, depth = grad.shape
    peers, _, half = near.shape
    lines = half // peers
    return pl.pallas_call(
        low_kernel,
        out_shape=pltpu.HBM((peers, 2 * roles * lines + 8, width), jnp.float32),
        in_specs=[VMEM, VMEM, VMEM, VMEM],
        out_specs=HBM,
        scratch_shapes=[
            pltpu.VMEM((2, roles, peers, lines, width), jnp.float32),
            pltpu.VMEM((peers, 8, width), jnp.float32),
            pltpu.SemaphoreType.DMA((2 * roles + 1,)),
        ],
        compiler_params=room(22),
        cost_estimate=cost(4 * roles * width * depth * 2 * half, 11 * 10**6),
        name="low_parts",
    )(grad, near, far, gate)


def sum_kernel(arrived_ref, out_ref, block, sems):
    block[...] = jnp.sum(arrived_ref[...], axis=0)
    peers = out_ref.shape[0]
    finished(started([(block, out_ref.at[peer]) for peer in range(peers)], sems))


def summed(arrived):
    return pl.pallas_call(
        sum_kernel,
        out_shape=pltpu.HBM(arrived.shape, jnp.float32),
        in_specs=[VMEM],
        out_specs=HBM,
        scratch_shapes=[
            pltpu.VMEM(arrived.shape[1:], jnp.float32),
            pltpu.SemaphoreType.DMA((arrived.shape[0],)),
        ],
        compiler_params=room(8),
        cost_estimate=cost(10**6, 2 * 10**6),
        name="summed",
    )(arrived)


def moment_kernel(
    place_ref, sums_ref, first_hbm, second_hbm, first_new_hbm, second_new_hbm, upper_hbm,
    lower_hbm, shared_hbm, first_ref, second_ref, upper_ref, lower_ref, message, read_sems,
    write_sems,
):
    core = place_ref[2]
    roles, rank, width = first_ref.shape
    peers = sums_ref.shape[0]
    half = rank // 2
    block = half // peers
    reads = [
        started(
            [(first_hbm.at[role], first_ref.at[role]), (second_hbm.at[role], second_ref.at[role])],
            read_sems.at[role],
        )
        for role in range(roles)
    ]
    squares = jnp.zeros((half, width), jnp.float32)
    writes = []
    for role in range(roles):
        finished(reads[role])
        for side in range(2):
            at = (side * roles + role) * block
            low = sums_ref[:, at : at + block, :].reshape(half, width)
            at = pl.ds(pl.multiple_of((core ^ side) * half, half), half)
            first_new = BETA_ONE * first_ref[role, at] + (1.0 - BETA_ONE) * low
            second_new = BETA_TWO * second_ref[role, at] + (1.0 - BETA_TWO) * low * low
            direction = first_new / jnp.sqrt(second_new)
            first_ref[role, at] = first_new
            second_ref[role, at] = second_new
            squares = squares + direction * direction
            upper, lower = halves(direction)
            upper_ref[role, side * half : (side + 1) * half] = upper
            lower_ref[role, side * half : (side + 1) * half] = lower
        made = [first_ref, second_ref, upper_ref, lower_ref]
        kept = [first_new_hbm, second_new_hbm, upper_hbm, lower_hbm]
        pairs = [(a.at[role], b.at[role]) for a, b in zip(made, kept)]
        writes += started(pairs, write_sems.at[pl.ds(role * 4, 4)])
    squares = jnp.sum(squares, axis=(0, 1), keepdims=True)
    heads = peers
    for head in range(heads):
        message[head : head + 1, :] = sums_ref[head, 6 * block : 6 * block + 1, :]
    message[heads:, :] = jnp.broadcast_to(squares, (8, width))
    copies = shared_hbm.shape[0]
    pairs = [(message, shared_hbm.at[copy]) for copy in range(copies)]
    finished(writes + started(pairs, write_sems.at[pl.ds(roles * 4, copies)]))


def moments(place, sums, first_moment, second_moment, copies):
    shape = first_moment.shape
    heads = sums.shape[0]
    return pl.pallas_call(
        moment_kernel,
        out_shape=[
            pltpu.HBM(shape, jnp.float32),
            pltpu.HBM(shape, jnp.float32),
            pltpu.HBM(shape, jnp.bfloat16),
            pltpu.HBM(shape, jnp.bfloat16),
            pltpu.HBM((copies, heads + 8, shape[2]), jnp.float32),
        ],
        in_specs=[SMEM, VMEM, HBM, HBM],
        out_specs=[HBM] * 5,
        scratch_shapes=[pltpu.VMEM(shape, jnp.float32)] * 2
        + [pltpu.VMEM(shape, jnp.bfloat16)] * 2
        + [
            pltpu.VMEM((heads + 8, shape[2]), jnp.float32),
            pltpu.SemaphoreType.DMA((shape[0], 2)),
            pltpu.SemaphoreType.DMA((shape[0] * 4 + copies,)),
        ],
        compiler_params=room(12),
        cost_estimate=cost(10**7, 6 * 10**6),
        name="moments",
    )(place, sums, *held(pltpu.HBM, first_moment, second_moment))


def product_kernel(
    near_hbm, far_hbm, upper_hbm, lower_hbm, out_hbm, factor_ref, direction_ref, product_ref,
    read_sems, write_sems,
):
    roles, peers, rows, rank = factor_ref.shape
    half = rank // 2

    def operands(role):
        lines = pl.ds(role * rows, rows)
        pairs = [
            (ref.at[:, lines, :], factor_ref.at[role, :, :, pl.ds(side * half, half)])
            for side, ref in enumerate((near_hbm, far_hbm))
        ]
        directions = enumerate((upper_hbm, lower_hbm))
        pairs += [(ref.at[role], direction_ref.at[role, n]) for n, ref in directions]
        return started(pairs, read_sems.at[role])

    reads = [operands(role) for role in range(roles)]
    writes = []
    for role in range(roles):
        finished(reads[role])
        factor = factor_ref[role].reshape(peers * rows, rank)
        product_ref[role] = jnp.dot(
            factor, direction_ref[role, 0], preferred_element_type=jnp.float32
        ) + jnp.dot(factor, direction_ref[role, 1], preferred_element_type=jnp.float32)
        pairs = [(product_ref.at[role], out_hbm.at[role])]
        writes += started(pairs, write_sems.at[pl.ds(role, 1)])
    finished(writes)


def products(near, far, upper, lower, rows):
    roles, rank, width = upper.shape
    peers = near.shape[0]
    shape = (roles, peers * rows, width)
    return pl.pallas_call(
        product_kernel,
        out_shape=pltpu.HBM(shape, jnp.float32),
        in_specs=[HBM] * 4,
        out_specs=HBM,
        scratch_shapes=[
            pltpu.VMEM((roles, peers, rows, rank), jnp.bfloat16),
            pltpu.VMEM((roles, 2, rank, width), jnp.bfloat16),
            pltpu.VMEM(shape, jnp.float32),
            pltpu.SemaphoreType.DMA((roles, 4)),
            pltpu.SemaphoreType.DMA((roles,)),
        ],
        compiler_params=room(20),
        cost_estimate=cost(4 * roles * peers * rows * rank * width, 10**7),
        name="products",
    )(*held(pltpu.HBM, near, far, upper, lower))


def final_kernel(entries, place_ref, product_hbm, *refs):
    pieces, shared_ref, inputs, outputs, refs = refs[:18], refs[18], refs[19:23], refs[23:30], refs[30:]
    count = 18 - len(NEXT)
    product_ref, piece_refs, refs = refs[0], list(refs[1 : count + 1]), refs[count + 1 :]
    kept, made, (piece_sems, rest_sems, write_sems) = refs[:4], refs[4:11], refs[11:]
    for n in NEXT:
        piece_refs.insert(n, pieces[n])
    master_ref, gate_master_ref, gate_first_ref, gate_second_ref = kept
    step_ref, new_ref, copy_ref, *gate_refs = made
    heads = gate_master_ref.shape[0]
    roles, rows, width = master_ref.shape
    rest = started(zip(inputs, kept), rest_sems)
    waits = []
    for role in range(roles):
        pairs = [(product_hbm.at[role], product_ref.at[role])]
        chosen, index = (range(0, 5), role) if role + 1 < roles else (range(5, 9), 0)
        for n in [part * 9 + n for part in range(2) for n in chosen if part * 9 + n not in NEXT]:
            pairs.append((pieces[n].at[:, index], piece_refs[n].at[:, index]))
        waits.append(started(pairs, piece_sems.at[role]))
    along = place_ref[3], place_ref[4]
    side = rows // 2
    own = pl.ds(pl.multiple_of(place_ref[0] * rows, rows), rows)
    finished(rest)
    squares = jnp.sum(shared_ref[:, heads, 0:1], axis=0, keepdims=True)
    scale = 1.0 / jnp.sqrt(squares / entries + 1e-06)
    writes = []
    for peer in range(shared_ref.shape[0]):
        at = slice(peer * width, (peer + 1) * width)
        grad = shared_ref[peer, :heads]
        first = BETA_ONE * gate_first_ref[:, at] + (1.0 - BETA_ONE) * grad
        second = BETA_TWO * gate_second_ref[:, at] + (1.0 - BETA_TWO) * grad * grad
        new = gate_master_ref[:, at] - LEARN * first / jnp.sqrt(second)
        gate_refs[0][:, at] = new
        gate_refs[1][:, at] = new.astype(jnp.bfloat16)
        gate_refs[2][:, at] = first
        gate_refs[3][:, at] = second
    writes += started(zip(made[3:], outputs[3:]), write_sems.at[pl.ds(roles * 3, 4)])
    for role in range(roles):
        finished(waits[role])
        for part in range(2):
            for first in range(4):
                for second in range(4):
                    offsets = (first, second) if part == 0 else (second, first)
                    source = [(along[n] + 4 - offsets[n]) % 4 for n in range(2)]
                    source = source[0] * 4 + source[1]
                    at = pl.ds(pl.multiple_of(source * rows + part * side, side), side)
                    index = first
                    if role + 1 == roles:
                        ref = piece_refs[part * 9 + 5 + second][index, 0]
                    else:
                        place = (0, 1, 3 + first // 2, 2)[second]
                        index = first % 2 if second == 2 else first
                        ref = piece_refs[part * 9 + place][index, role]
                    new = ref - LEARN * (scale * product_ref[role, at])
                    copy_ref[role, at] = new.astype(jnp.bfloat16)
        step = scale * product_ref[role, own]
        step_ref[role] = step
        new_ref[role] = master_ref[role] - LEARN * step
        pairs = [(made[n].at[role], outputs[n].at[role]) for n in range(3)]
        writes += started(pairs, write_sems.at[pl.ds(role * 3, 3)])
    finished(writes)


def finals(entries, place, product, pieces, shared, master, gates):
    roles = master.shape[0]
    outs = [
        (master.shape, jnp.float32),
        (master.shape, jnp.float32),
        (product.shape, jnp.bfloat16),
        (gates[0].shape, jnp.float32),
        (gates[0].shape, jnp.bfloat16),
        (gates[0].shape, jnp.float32),
        (gates[0].shape, jnp.float32),
    ]
    inputs = (master, *gates)
    copied = [piece for n, piece in enumerate(pieces) if n not in NEXT]
    kept = [(a.shape, a.dtype) for a in (product, *copied, *inputs)]
    pieces = [a if n in NEXT else held(pltpu.HBM, a)[0] for n, a in enumerate(pieces)]
    specs = [VMEM if n in NEXT else HBM for n in range(len(pieces))]
    dma = pltpu.SemaphoreType.DMA
    return pl.pallas_call(
        functools.partial(final_kernel, entries),
        out_shape=[pltpu.HBM(*out) for out in outs],
        in_specs=[SMEM, HBM, *specs, VMEM] + [HBM] * len(inputs),
        out_specs=[HBM] * 7,
        scratch_shapes=[pltpu.VMEM(*a) for a in kept + outs]
        + [dma((roles, 11)), dma((4,)), dma((roles * 3 + 4,))],
        compiler_params=room(32),
        cost_estimate=cost(10**7, 16 * 10**6),
        name="finals",
    )(place, *held(pltpu.HBM, product), *pieces, shared, *held(pltpu.HBM, *inputs))


def join_kernel(master_hbm, *refs):
    pieces, outs, blocks, (read_sems, write_sems) = refs[:6], refs[6:10], refs[10:12], refs[12:]
    early = outs[0].shape[1]
    side = master_hbm.shape[1] // 2
    pairs = []
    for part, block in enumerate(blocks):
        pairs.append((master_hbm.at[:, pl.ds(part * side, side)], block.at[0]))
        pairs += [(pieces[part * 3 + n].at[0], block.at[n + 1]) for n in range(3)]
    reads, writes = started(pairs, read_sems), []
    for n, read in enumerate(reads):
        read.wait()
        block = blocks[n // 4].at[n % 4]
        pairs = [
            (block.at[pl.ds(0, early)], outs[n // 4].at[n % 4]),
            (block.at[pl.ds(early, block.shape[0] - early)], outs[2 + n // 4].at[n % 4]),
        ]
        writes += started(pairs, write_sems.at[pl.ds(n * 2, 2)])
    finished(writes)


def joined(master, pieces, early):
    shape = (4, *pieces[0].shape[1:])
    return pl.pallas_call(
        join_kernel,
        out_shape=[
            pltpu.HBM((4, count, *shape[2:]), jnp.float32)
            for count in (early, early, shape[1] - early, shape[1] - early)
        ],
        in_specs=[HBM] * 7,
        out_specs=[HBM] * 4,
        scratch_shapes=[pltpu.VMEM(shape, jnp.float32)] * 2
        + [pltpu.SemaphoreType.DMA((8,)), pltpu.SemaphoreType.DMA((16,))],
        compiler_params=room(4),
        cost_estimate=cost(10**6, 6 * 10**6),
        name="joined",
    )(*held(pltpu.HBM, master, *pieces))


def shift(x, axis, by):
    return lax.ppermute(x, axis, [(i, (i + by) % 4) for i in range(4)])


def local(
    saved_input,
    proj_cot,
    log_cache,
    cache_cot,
    proj_master,
    factors,
    first_moment,
    second_moment,
    gate_master,
    gate_first,
    gate_second,
):
    roles, rows, _ = factors.shape
    width = proj_cot.shape[2]
    peers = lax.axis_size(FS)
    place = [lax.axis_index(name) for name in (FS, TP, "c", "z", "x")]
    place = jnp.stack(place).astype(jnp.int32)

    near = packed(place, factors, log_cache, cache_cot, peers)
    near = lax.all_to_all(near, FS, split_axis=0, concat_axis=0, tiled=True)
    far = lax.ppermute(near, "c", [(0, 1), (1, 0)])
    sides = proj_master.reshape(roles, 2, rows // 2, width)
    spread = [
        shift(sides[:, part][None], axis, by) for part, axis in enumerate(FS) for by in (1, 2, 3)
    ]
    axes = FS[::-1]
    *early, first_late, second_late = joined(proj_master, spread, roles - 1)
    late = (first_late, second_late)
    ahead = [shift(side, axis, 1) for side, axis in zip(early, axes)]
    behind = [shift(side, axis, 3) for side, axis in zip(early, axes)]
    opposite = [side[:2] for side in ahead]
    other = [side[2:] for side in behind]
    opposite = [shift(side, axis, 1) for side, axis in zip(opposite, axes)]
    other = [shift(side, axis, 3) for side, axis in zip(other, axes)]
    late = [[side] + [shift(side, axis, by) for by in (1, 2, 3)] for side, axis in zip(late, axes)]
    pieces = [
        [*group, *rest] for *group, rest in zip(early, ahead, behind, opposite, other, late)
    ]
    pieces = [piece for group in pieces for piece in group]
    grad = jnp.einsum("td,rtw->rwd", saved_input, proj_cot, preferred_element_type=jnp.float32)
    gate_part = gate_columns(place, log_cache, cache_cot, near, saved_input, width)
    parts = low_parts(grad, near, far, gate_part)
    arrived = lax.all_to_all(parts, FS, split_axis=0, concat_axis=0, tiled=True)
    sums = lax.all_to_all(summed(arrived), FS, split_axis=0, concat_axis=0, tiled=True)

    first_new, second_new, upper, lower, shared = moments(
        place, sums, first_moment, second_moment, lax.axis_size(TP)
    )
    shared = lax.all_to_all(shared, TP, split_axis=0, concat_axis=0, tiled=True)
    product = products(near, far, upper, lower, rows)
    entries = first_new.size * lax.axis_size(TP)
    gates = (gate_master, gate_first, gate_second)
    step, new, copy, *gates = finals(entries, place, product, pieces, shared, proj_master, gates)
    return step, new, copy, first_new, second_new, *gates


def solution(mesh):
    fine = Mesh(mesh.devices.reshape(4, 4, 4, 2), (*FS, *TP))
    placed = (
        P(FS, None),
        P(None, FS, TP),
        P(None, FS),
        P(None, FS),
        P(None, FS, TP),
        P(None, FS, None),
        P(None, None, TP),
        P(None, None, TP),
        P(),
        P(),
        P(),
    )

    return jax.shard_map(
        local,
        mesh=fine,
        in_specs=placed,
        out_specs=(
            P(None, FS, TP),
            P(None, FS, TP),
            P(None, None, TP),
            P(None, None, TP),
            P(None, None, TP),
            P(),
            P(),
            P(),
            P(),
        ),
        check_vma=False,
    )
```

```python
import functools

import jax
import jax.numpy as jnp
from jax import lax
from jax.experimental import pallas as pl
from jax.experimental.pallas import tpu as pltpu
from jax.sharding import Mesh
from jax.sharding import PartitionSpec as P

BETA_ONE = 0.8
BETA_TWO = 0.9
LEARN = 0.001
FS = ("z", "x")
NEXT = (1, 2, 10, 11)
TP = ("y", "c")


VMEM = pl.BlockSpec(memory_space=pltpu.VMEM)
SMEM = pl.BlockSpec(memory_space=pltpu.SMEM)
HBM = pl.BlockSpec(memory_space=pltpu.HBM)


def room(mebibytes):
    return pltpu.CompilerParams(vmem_limit_bytes=mebibytes * 2**20)


def held(space, *arrays):
    return [pltpu.with_memory_space_constraint(a, space) for a in arrays]


def cost(flops, moved):
    return pl.CostEstimate(flops=flops, bytes_accessed=moved, transcendentals=0)


def halves(x):
    upper = x.astype(jnp.bfloat16)
    return upper, (x - upper.astype(jnp.float32)).astype(jnp.bfloat16)


def started(pairs, sems):
    copies = [pltpu.make_async_copy(a, b, sems.at[n]) for n, (a, b) in enumerate(pairs)]
    for copy in copies:
        copy.start()
    return copies


def finished(copies):
    for copy in copies:
        copy.wait()


def pack_kernel(
    place_ref, factor_ref, log_ref, cot_ref, out_ref, last, cot, block, read_sems, write_sems
):
    peers, lines, lanes = out_ref.shape
    heads, length = log_ref.shape
    roles, rows, _ = factor_ref.shape
    at = pl.ds(pl.multiple_of(place_ref[2] * lanes, lanes), lanes)
    reads = [(factor_ref.at[r, :, at], block.at[pl.ds(r * rows, rows)]) for r in range(roles)]
    reads += [(log_ref.at[:, pl.ds(length - lanes, lanes)], last), (cot_ref, cot)]
    reads = started(reads, read_sems)
    finished(reads[:roles])
    body, rest_of = pl.ds(0, roles * rows), pl.ds(roles * rows, lines - roles * rows)
    pairs = [(block.at[body], out_ref.at[peer, body]) for peer in range(peers)]
    writes = started(pairs, write_sems.at[pl.ds(0, peers)])
    finished(reads[roles:])
    column = lax.broadcasted_iota(jnp.int32, (heads, lanes), 1)
    row = lax.broadcasted_iota(jnp.int32, (heads, lanes), 0)
    totals = jnp.sum(cot[...], axis=1, keepdims=True)
    ends = jnp.where(column == row, totals, 0.0)
    ends = ends + jnp.where(column == row + heads, last[:, lanes - 1 :], 0.0)
    ends = jnp.sum(ends, axis=0, keepdims=True)
    upper, lower = halves(ends)
    rest = ends - upper.astype(jnp.float32)
    rest = rest - lower.astype(jnp.float32)
    line = lax.broadcasted_iota(jnp.int32, (lines - roles * rows, lanes), 0)
    tail = jnp.where(line == 0, upper.astype(jnp.float32), 0.0)
    tail = jnp.where(line == 1, lower.astype(jnp.float32), tail)
    tail = jnp.where(line == 2, rest, tail).astype(jnp.bfloat16)
    block[roles * rows :, :] = tail
    pairs = [(block.at[rest_of], out_ref.at[peer, rest_of]) for peer in range(peers)]
    finished(writes + started(pairs, write_sems.at[pl.ds(peers, peers)]))


def packed(place, factors, log_cache, cache_cot, peers):
    roles, rows, rank = factors.shape
    heads, length = log_cache.shape
    lanes = rank // 2
    lines = roles * rows + 16
    return pl.pallas_call(
        pack_kernel,
        out_shape=pltpu.HBM((peers, lines, lanes), jnp.bfloat16),
        in_specs=[SMEM, HBM, HBM, HBM],
        out_specs=HBM,
        scratch_shapes=[
            pltpu.VMEM((heads, lanes), jnp.float32),
            pltpu.VMEM((heads, length), jnp.float32),
            pltpu.VMEM((lines, lanes), jnp.bfloat16),
            pltpu.SemaphoreType.DMA((roles + 2,)),
            pltpu.SemaphoreType.DMA((2 * peers,)),
        ],
        compiler_params=room(8),
        cost_estimate=cost(10**6, 2 * 10**6),
        name="packed",
    )(place, *held(pltpu.HBM, factors, log_cache, cache_cot))


def gate_kernel(
    place_ref, log_hbm, cot_hbm, ends_hbm, input_hbm, out_ref, log_ref, cot_ref, ends_ref,
    input_ref, sems,
):
    lines, width = ends_hbm.shape[1], input_ref.shape[1]
    at = pl.ds(pl.multiple_of(place_ref[1] * width, width), width)
    reads = [
        (log_hbm, log_ref),
        (cot_hbm, cot_ref),
        (ends_hbm.at[:, pl.ds(lines - 16, 16)], ends_ref),
        (input_hbm.at[:, at], input_ref),
    ]
    reads = started(reads, sems)
    finished(reads[:3])
    me = place_ref[0]
    heads, length = log_ref.shape
    ends = ends_ref[...].astype(jnp.float32)
    ends = ends[:, 0, :] + ends[:, 1, :] + ends[:, 2, :]
    source = lax.broadcasted_iota(jnp.int32, ends.shape, 0)
    after = jnp.sum(jnp.where(source > me, ends, 0.0), axis=0, keepdims=True)
    before = jnp.sum(jnp.where(source == me - 1, ends, 0.0), axis=0, keepdims=True)
    lane = lax.broadcasted_iota(jnp.int32, (heads, ends.shape[1]), 1)
    row = lax.broadcasted_iota(jnp.int32, (heads, ends.shape[1]), 0)
    carried = jnp.sum(jnp.where(lane == row, after, 0.0), axis=1, keepdims=True)
    edge = jnp.sum(jnp.where(lane == row + heads, before, 0.0), axis=1, keepdims=True)
    place = lax.broadcasted_iota(jnp.int32, (heads, length), 1)
    total = cot_ref[...]
    step = 1
    while step < length:
        total = total + jnp.where(place < length - step, pltpu.roll(total, length - step, 1), 0.0)
        step *= 2
    log = log_ref[...]
    previous = jnp.where(place == 0, edge, pltpu.roll(log, 1, 1))
    delta = log - previous
    closed = -jnp.tanh(0.5 * delta) * (jnp.exp(delta) + 1.0)
    gate_cot = ((total + carried) * closed).astype(jnp.bfloat16)
    finished(reads[3:])
    out_ref[...] = jnp.dot(gate_cot, input_ref[...], preferred_element_type=jnp.float32)


def gate_columns(place, log_cache, cache_cot, ends, saved_input, width):
    heads, length = log_cache.shape
    peers, _, lanes = ends.shape
    return pl.pallas_call(
        gate_kernel,
        out_shape=jax.ShapeDtypeStruct((heads, width), jnp.float32),
        in_specs=[SMEM, HBM, HBM, pl.BlockSpec(memory_space=pl.ANY), HBM],
        out_specs=VMEM,
        scratch_shapes=[
            pltpu.VMEM((heads, length), jnp.float32),
            pltpu.VMEM((heads, length), jnp.float32),
            pltpu.VMEM((peers, 16, lanes), jnp.bfloat16),
            pltpu.VMEM((length, width), jnp.bfloat16),
            pltpu.SemaphoreType.DMA((4,)),
        ],
        compiler_params=room(10),
        cost_estimate=cost(4 * 10**9, 4 * 10**6),
        name="gate_columns",
    )(place, *held(pltpu.HBM, log_cache, cache_cot), ends, *held(pltpu.HBM, saved_input))


def low_kernel(
    grad_ref, near_ref, far_ref, gate_ref, out_hbm, out_ref, tail_ref, write_sems,
):
    roles, width, depth = grad_ref.shape
    peers, _, half = near_ref.shape
    rows = depth // peers
    lines = half // peers
    tail_ref[...] = jnp.zeros_like(tail_ref)
    for head in range(gate_ref.shape[0]):
        tail_ref[head, 0:1, :] = gate_ref[head : head + 1, :]
    writes = [(tail_ref, out_hbm.at[:, pl.ds(2 * roles * lines, tail_ref.shape[1])])]
    writes = started(writes, write_sems.at[pl.ds(2 * roles, 1)])
    for role in range(roles):
        at = slice(role * rows, (role + 1) * rows)
        sides = [ref[:, at, :].reshape(depth, half) for ref in (near_ref, far_ref)]
        pieces = jnp.concatenate(sides, axis=1)
        both = jnp.concatenate(halves(grad_ref[role]), axis=0)
        low = jnp.dot(both, pieces, preferred_element_type=jnp.float32)
        low = (low[:width] + low[width:]).T
        pairs = []
        for side in range(2):
            part = low[side * half : (side + 1) * half].reshape(peers, lines, width)
            out_ref[side, role] = part
            place = pl.ds((side * roles + role) * lines, lines)
            pairs.append((out_ref.at[side, role], out_hbm.at[:, place]))
        writes += started(pairs, write_sems.at[pl.ds(2 * role, 2)])
    finished(writes)


def low_parts(grad, near, far, gate):
    roles, width, depth = grad.shape
    peers, _, half = near.shape
    lines = half // peers
    return pl.pallas_call(
        low_kernel,
        out_shape=pltpu.HBM((peers, 2 * roles * lines + 8, width), jnp.float32),
        in_specs=[VMEM, VMEM, VMEM, VMEM],
        out_specs=HBM,
        scratch_shapes=[
            pltpu.VMEM((2, roles, peers, lines, width), jnp.float32),
            pltpu.VMEM((peers, 8, width), jnp.float32),
            pltpu.SemaphoreType.DMA((2 * roles + 1,)),
        ],
        compiler_params=room(22),
        cost_estimate=cost(4 * roles * width * depth * 2 * half, 11 * 10**6),
        name="low_parts",
    )(grad, near, far, gate)


def sum_kernel(arrived_ref, out_ref, block, sems):
    block[...] = jnp.sum(arrived_ref[...], axis=0)
    peers = out_ref.shape[0]
    finished(started([(block, out_ref.at[peer]) for peer in range(peers)], sems))


def summed(arrived):
    return pl.pallas_call(
        sum_kernel,
        out_shape=pltpu.HBM(arrived.shape, jnp.float32),
        in_specs=[VMEM],
        out_specs=HBM,
        scratch_shapes=[
            pltpu.VMEM(arrived.shape[1:], jnp.float32),
            pltpu.SemaphoreType.DMA((arrived.shape[0],)),
        ],
        compiler_params=room(8),
        cost_estimate=cost(10**6, 2 * 10**6),
        name="summed",
    )(arrived)


def moment_kernel(
    place_ref, sums_ref, first_hbm, second_hbm, first_new_hbm, second_new_hbm, upper_hbm,
    lower_hbm, shared_hbm, first_ref, second_ref, upper_ref, lower_ref, message, read_sems,
    write_sems,
):
    core = place_ref[2]
    roles, rank, width = first_ref.shape
    peers = sums_ref.shape[0]
    half = rank // 2
    block = half // peers
    reads = [
        started(
            [(first_hbm.at[role], first_ref.at[role]), (second_hbm.at[role], second_ref.at[role])],
            read_sems.at[role],
        )
        for role in range(roles)
    ]
    squares = jnp.zeros((half, width), jnp.float32)
    writes = []
    for role in range(roles):
        finished(reads[role])
        for side in range(2):
            at = (side * roles + role) * block
            low = sums_ref[:, at : at + block, :].reshape(half, width)
            at = pl.ds(pl.multiple_of((core ^ side) * half, half), half)
            first_new = BETA_ONE * first_ref[role, at] + (1.0 - BETA_ONE) * low
            second_new = BETA_TWO * second_ref[role, at] + (1.0 - BETA_TWO) * low * low
            direction = first_new / jnp.sqrt(second_new)
            first_ref[role, at] = first_new
            second_ref[role, at] = second_new
            squares = squares + direction * direction
            upper, lower = halves(direction)
            upper_ref[role, side * half : (side + 1) * half] = upper
            lower_ref[role, side * half : (side + 1) * half] = lower
        made = [first_ref, second_ref, upper_ref, lower_ref]
        kept = [first_new_hbm, second_new_hbm, upper_hbm, lower_hbm]
        pairs = [(a.at[role], b.at[role]) for a, b in zip(made, kept)]
        writes += started(pairs, write_sems.at[pl.ds(role * 4, 4)])
    squares = jnp.sum(squares, axis=(0, 1), keepdims=True)
    heads = peers
    for head in range(heads):
        message[head : head + 1, :] = sums_ref[head, 6 * block : 6 * block + 1, :]
    message[heads:, :] = jnp.broadcast_to(squares, (8, width))
    copies = shared_hbm.shape[0]
    pairs = [(message, shared_hbm.at[copy]) for copy in range(copies)]
    finished(writes + started(pairs, write_sems.at[pl.ds(roles * 4, copies)]))


def moments(place, sums, first_moment, second_moment, copies):
    shape = first_moment.shape
    heads = sums.shape[0]
    return pl.pallas_call(
        moment_kernel,
        out_shape=[
            pltpu.HBM(shape, jnp.float32),
            pltpu.HBM(shape, jnp.float32),
            pltpu.HBM(shape, jnp.bfloat16),
            pltpu.HBM(shape, jnp.bfloat16),
            pltpu.HBM((copies, heads + 8, shape[2]), jnp.float32),
        ],
        in_specs=[SMEM, VMEM, HBM, HBM],
        out_specs=[HBM] * 5,
        scratch_shapes=[pltpu.VMEM(shape, jnp.float32)] * 2
        + [pltpu.VMEM(shape, jnp.bfloat16)] * 2
        + [
            pltpu.VMEM((heads + 8, shape[2]), jnp.float32),
            pltpu.SemaphoreType.DMA((shape[0], 2)),
            pltpu.SemaphoreType.DMA((shape[0] * 4 + copies,)),
        ],
        compiler_params=room(12),
        cost_estimate=cost(10**7, 6 * 10**6),
        name="moments",
    )(place, sums, *held(pltpu.HBM, first_moment, second_moment))


def product_kernel(
    near_hbm, far_hbm, upper_hbm, lower_hbm, out_hbm, factor_ref, direction_ref, product_ref,
    read_sems, write_sems,
):
    roles, peers, rows, rank = factor_ref.shape
    half = rank // 2

    def operands(role):
        lines = pl.ds(role * rows, rows)
        pairs = [
            (ref.at[:, lines, :], factor_ref.at[role, :, :, pl.ds(side * half, half)])
            for side, ref in enumerate((near_hbm, far_hbm))
        ]
        directions = enumerate((upper_hbm, lower_hbm))
        pairs += [(ref.at[role], direction_ref.at[role, n]) for n, ref in directions]
        return started(pairs, read_sems.at[role])

    reads = [operands(role) for role in range(roles)]
    writes = []
    for role in range(roles):
        finished(reads[role])
        for part in range(2):
            at = slice(part * peers // 2, (part + 1) * peers // 2)
            factor = factor_ref[role, at].reshape(peers * rows // 2, rank)
            at = pl.ds(part * peers * rows // 2, peers * rows // 2)
            product_ref[role, at] = jnp.dot(
                factor, direction_ref[role, 0], preferred_element_type=jnp.float32
            ) + jnp.dot(factor, direction_ref[role, 1], preferred_element_type=jnp.float32)
            pairs = [(product_ref.at[role, at], out_hbm.at[role, at])]
            writes += started(pairs, write_sems.at[pl.ds(role * 2 + part, 1)])
    finished(writes)


def products(near, far, upper, lower, rows):
    roles, rank, width = upper.shape
    peers = near.shape[0]
    shape = (roles, peers * rows, width)
    return pl.pallas_call(
        product_kernel,
        out_shape=pltpu.HBM(shape, jnp.float32),
        in_specs=[HBM] * 4,
        out_specs=HBM,
        scratch_shapes=[
            pltpu.VMEM((roles, peers, rows, rank), jnp.bfloat16),
            pltpu.VMEM((roles, 2, rank, width), jnp.bfloat16),
            pltpu.VMEM(shape, jnp.float32),
            pltpu.SemaphoreType.DMA((roles, 4)),
            pltpu.SemaphoreType.DMA((roles * 2,)),
        ],
        compiler_params=room(20),
        cost_estimate=cost(4 * roles * peers * rows * rank * width, 10**7),
        name="products",
    )(*held(pltpu.HBM, near, far, upper, lower))


def final_kernel(entries, place_ref, product_hbm, *refs):
    pieces, shared_ref, inputs, outputs, refs = refs[:18], refs[18], refs[19:23], refs[23:30], refs[30:]
    count = 18 - len(NEXT)
    product_ref, piece_refs, refs = refs[0], list(refs[1 : count + 1]), refs[count + 1 :]
    kept, made, (piece_sems, rest_sems, write_sems) = refs[:4], refs[4:11], refs[11:]
    for n in NEXT:
        piece_refs.insert(n, pieces[n])
    master_ref, gate_master_ref, gate_first_ref, gate_second_ref = kept
    step_ref, new_ref, copy_ref, *gate_refs = made
    heads = gate_master_ref.shape[0]
    roles, rows, width = master_ref.shape
    rest = started(zip(inputs, kept), rest_sems)
    waits = []
    for role in range(roles):
        pairs = [(product_hbm.at[role], product_ref.at[role])]
        chosen, index = (range(0, 5), role) if role + 1 < roles else (range(5, 9), 0)
        for n in [part * 9 + n for part in range(2) for n in chosen if part * 9 + n not in NEXT]:
            pairs.append((pieces[n].at[:, index], piece_refs[n].at[:, index]))
        waits.append(started(pairs, piece_sems.at[role]))
    along = place_ref[3], place_ref[4]
    side = rows // 2
    own = pl.ds(pl.multiple_of(place_ref[0] * rows, rows), rows)
    finished(rest)
    squares = jnp.sum(shared_ref[:, heads, 0:1], axis=0, keepdims=True)
    scale = 1.0 / jnp.sqrt(squares / entries + 1e-06)
    writes = []
    for peer in range(shared_ref.shape[0]):
        at = slice(peer * width, (peer + 1) * width)
        grad = shared_ref[peer, :heads]
        first = BETA_ONE * gate_first_ref[:, at] + (1.0 - BETA_ONE) * grad
        second = BETA_TWO * gate_second_ref[:, at] + (1.0 - BETA_TWO) * grad * grad
        new = gate_master_ref[:, at] - LEARN * first / jnp.sqrt(second)
        gate_refs[0][:, at] = new
        gate_refs[1][:, at] = new.astype(jnp.bfloat16)
        gate_refs[2][:, at] = first
        gate_refs[3][:, at] = second
    writes += started(zip(made[3:], outputs[3:]), write_sems.at[pl.ds(roles * 3, 4)])
    for role in range(roles):
        finished(waits[role])
        for part in range(2):
            for first in range(4):
                for second in range(4):
                    offsets = (first, second) if part == 0 else (second, first)
                    source = [(along[n] + 4 - offsets[n]) % 4 for n in range(2)]
                    source = source[0] * 4 + source[1]
                    at = pl.ds(pl.multiple_of(source * rows + part * side, side), side)
                    index = first
                    if role + 1 == roles:
                        ref = piece_refs[part * 9 + 5 + second][index, 0]
                    else:
                        place = (0, 1, 3 + first // 2, 2)[second]
                        index = first % 2 if second == 2 else first
                        ref = piece_refs[part * 9 + place][index, role]
                    new = ref - LEARN * (scale * product_ref[role, at])
                    copy_ref[role, at] = new.astype(jnp.bfloat16)
        step = scale * product_ref[role, own]
        step_ref[role] = step
        new_ref[role] = master_ref[role] - LEARN * step
        pairs = [(made[n].at[role], outputs[n].at[role]) for n in range(3)]
        writes += started(pairs, write_sems.at[pl.ds(role * 3, 3)])
    finished(writes)


def finals(entries, place, product, pieces, shared, master, gates):
    roles = master.shape[0]
    outs = [
        (master.shape, jnp.float32),
        (master.shape, jnp.float32),
        (product.shape, jnp.bfloat16),
        (gates[0].shape, jnp.float32),
        (gates[0].shape, jnp.bfloat16),
        (gates[0].shape, jnp.float32),
        (gates[0].shape, jnp.float32),
    ]
    inputs = (master, *gates)
    copied = [piece for n, piece in enumerate(pieces) if n not in NEXT]
    kept = [(a.shape, a.dtype) for a in (product, *copied, *inputs)]
    pieces = [a if n in NEXT else held(pltpu.HBM, a)[0] for n, a in enumerate(pieces)]
    specs = [VMEM if n in NEXT else HBM for n in range(len(pieces))]
    dma = pltpu.SemaphoreType.DMA
    return pl.pallas_call(
        functools.partial(final_kernel, entries),
        out_shape=[pltpu.HBM(*out) for out in outs],
        in_specs=[SMEM, HBM, *specs, VMEM] + [HBM] * len(inputs),
        out_specs=[HBM] * 7,
        scratch_shapes=[pltpu.VMEM(*a) for a in kept + outs]
        + [dma((roles, 11)), dma((4,)), dma((roles * 3 + 4,))],
        compiler_params=room(32),
        cost_estimate=cost(10**7, 16 * 10**6),
        name="finals",
    )(place, *held(pltpu.HBM, product), *pieces, shared, *held(pltpu.HBM, *inputs))


def join_kernel(master_hbm, *refs):
    pieces, outs, blocks, (read_sems, write_sems) = refs[:6], refs[6:10], refs[10:12], refs[12:]
    early = outs[0].shape[1]
    side = master_hbm.shape[1] // 2
    pairs = []
    for part, block in enumerate(blocks):
        pairs.append((master_hbm.at[:, pl.ds(part * side, side)], block.at[0]))
        pairs += [(pieces[part * 3 + n].at[0], block.at[n + 1]) for n in range(3)]
    reads, writes = started(pairs, read_sems), []
    for n, read in enumerate(reads):
        read.wait()
        block = blocks[n // 4].at[n % 4]
        pairs = [
            (block.at[pl.ds(0, early)], outs[n // 4].at[n % 4]),
            (block.at[pl.ds(early, block.shape[0] - early)], outs[2 + n // 4].at[n % 4]),
        ]
        writes += started(pairs, write_sems.at[pl.ds(n * 2, 2)])
    finished(writes)


def joined(master, pieces, early):
    shape = (4, *pieces[0].shape[1:])
    return pl.pallas_call(
        join_kernel,
        out_shape=[
            pltpu.HBM((4, count, *shape[2:]), jnp.float32)
            for count in (early, early, shape[1] - early, shape[1] - early)
        ],
        in_specs=[HBM] * 7,
        out_specs=[HBM] * 4,
        scratch_shapes=[pltpu.VMEM(shape, jnp.float32)] * 2
        + [pltpu.SemaphoreType.DMA((8,)), pltpu.SemaphoreType.DMA((16,))],
        compiler_params=room(4),
        cost_estimate=cost(10**6, 6 * 10**6),
        name="joined",
    )(*held(pltpu.HBM, master, *pieces))


def shift(x, axis, by):
    return lax.ppermute(x, axis, [(i, (i + by) % 4) for i in range(4)])


def local(
    saved_input,
    proj_cot,
    log_cache,
    cache_cot,
    proj_master,
    factors,
    first_moment,
    second_moment,
    gate_master,
    gate_first,
    gate_second,
):
    roles, rows, _ = factors.shape
    width = proj_cot.shape[2]
    peers = lax.axis_size(FS)
    place = [lax.axis_index(name) for name in (FS, TP, "c", "z", "x")]
    place = jnp.stack(place).astype(jnp.int32)

    near = packed(place, factors, log_cache, cache_cot, peers)
    near = lax.all_to_all(near, FS, split_axis=0, concat_axis=0, tiled=True)
    far = lax.ppermute(near, "c", [(0, 1), (1, 0)])
    sides = proj_master.reshape(roles, 2, rows // 2, width)
    spread = [
        shift(sides[:, part][None], axis, by) for part, axis in enumerate(FS) for by in (1, 2, 3)
    ]
    axes = FS[::-1]
    *early, first_late, second_late = joined(proj_master, spread, roles - 1)
    late = (first_late, second_late)
    ahead = [shift(side, axis, 1) for side, axis in zip(early, axes)]
    behind = [shift(side, axis, 3) for side, axis in zip(early, axes)]
    opposite = [side[:2] for side in ahead]
    other = [side[2:] for side in behind]
    opposite = [shift(side, axis, 1) for side, axis in zip(opposite, axes)]
    other = [shift(side, axis, 3) for side, axis in zip(other, axes)]
    late = [[side] + [shift(side, axis, by) for by in (1, 2, 3)] for side, axis in zip(late, axes)]
    pieces = [
        [*group, *rest] for *group, rest in zip(early, ahead, behind, opposite, other, late)
    ]
    pieces = [piece for group in pieces for piece in group]
    grad = jnp.einsum("td,rtw->rwd", saved_input, proj_cot, preferred_element_type=jnp.float32)
    gate_part = gate_columns(place, log_cache, cache_cot, near, saved_input, width)
    parts = low_parts(grad, near, far, gate_part)
    arrived = lax.all_to_all(parts, FS, split_axis=0, concat_axis=0, tiled=True)
    sums = lax.all_to_all(summed(arrived), FS, split_axis=0, concat_axis=0, tiled=True)

    first_new, second_new, upper, lower, shared = moments(
        place, sums, first_moment, second_moment, lax.axis_size(TP)
    )
    shared = lax.all_to_all(shared, TP, split_axis=0, concat_axis=0, tiled=True)
    product = products(near, far, upper, lower, rows)
    entries = first_new.size * lax.axis_size(TP)
    gates = (gate_master, gate_first, gate_second)
    step, new, copy, *gates = finals(entries, place, product, pieces, shared, proj_master, gates)
    return step, new, copy, first_new, second_new, *gates


def solution(mesh):
    fine = Mesh(mesh.devices.reshape(4, 4, 4, 2), (*FS, *TP))
    placed = (
        P(FS, None),
        P(None, FS, TP),
        P(None, FS),
        P(None, FS),
        P(None, FS, TP),
        P(None, FS, None),
        P(None, None, TP),
        P(None, None, TP),
        P(),
        P(),
        P(),
    )

    return jax.shard_map(
        local,
        mesh=fine,
        in_specs=placed,
        out_specs=(
            P(None, FS, TP),
            P(None, FS, TP),
            P(None, None, TP),
            P(None, None, TP),
            P(None, None, TP),
            P(),
            P(),
            P(),
            P(),
        ),
        check_vma=False,
    )
```
